256 devices in a mesh: grp: 2 (over y), sp: 32 (over z, core), tp: 4 (over x).
Axes of the slice: x: 4, y: 2, z: 16, core: 2. Of those that a mesh axis runs over, the one named last changes fastest.
The devices are a block of a 4x16x16 slice.
Arguments:
- queries: bfloat16 [8192, 2048], P(('grp', 'sp'), 'tp'), parts along dimension 0, may hold values from -8 to 8
- keys: bfloat16 [8192, 1024], P(('grp', 'sp'), 'tp'), parts along dimension 0, may hold values from -6 to 6
- values: bfloat16 [8192, 1024], P(('grp', 'sp'), 'tp'), parts along dimension 0, may hold values from -6 to 6
- head_bias: float32 [16], P('tp'), may hold values from -15 to -5
- documents: int32 [8192], P(('grp', 'sp')), parts along dimension 0, may hold values from 0 to 2, never falling along the last dimension, each value on 1 to 3072 neighbouring positions
- w_out: bfloat16 [2048, 2048], P('tp'), may hold values from -0.125 to 0.125
- resid: bfloat16 [8192, 2048], P(('grp', 'sp', 'tp')), parts along dimension 0, may hold values from -6 to 6
- norm_gain: float32 [2048], replicated, may hold values from 0.1 to 1.9
- expert_ids: int32 [8192, 2], P(('grp', 'sp', 'tp')), parts along dimension 0, may hold values from 0 to 31, all different within a row; in each aligned block of 32 rows (0 to 31, 32 to 63, ...) at most 4 rows name the same one
- expert_gates: float32 [8192, 2], P(('grp', 'sp', 'tp')), parts along dimension 0, may hold values from 0.1 to 0.9
- w_gate: bfloat16 [32, 2048, 3072], P('sp', None, 'tp'), may hold values from -0.125 to 0.125
- w_up: bfloat16 [32, 2048, 3072], P('sp', None, 'tp'), may hold values from -0.125 to 0.125
- w_down: bfloat16 [32, 3072, 2048], P('sp', 'tp'), may hold values from -0.109375 to 0.109375
Outputs:
- layer_out: bfloat16 [8192, 2048], P(('grp', 'sp', 'tp')), parts along dimension 0
The draws below stay inside these ranges and needn't reach their ends.
There are 2 independent parts, one for each index of `grp`. The reference program is written for one: setup_inputs(seed, part) draws one part's arguments, and reference() takes and returns one part's arrays. A program takes and returns all parts, laid end to end along the dimension named above; an argument that names none is the same for every part. Nothing has to cross between parts.
Inputs may be any that keep to these rules, and one draw needn't show every extreme that they name: Document numbers never fall along the sequence; each of the 3 documents holds at least one position and the longest exactly 3072 positions. `expert_ids`: each position names 2 different experts. Among the 32 positions of one device (aligned blocks of 32 rows) no expert is named more than 4 times, and in some block some expert exactly 4 times.
All inputs are finite; a program needn't handle non-finite values.
Results may differ from the reference program's by a relative error of at most 0.012.
Values may be sent and summed in bfloat16 or wider, within the bound.
A program may use at most 64 MiB of HBM per device.

```python
import math
import jax
import jax.numpy as jnp
import numpy as np
from jax import lax

D = 2048
HEADS = 16
KV_HEADS = 8
DH = 128
FF = 3072
TOPK = 2
DOCS = 3
SEQ = 4096
ROWS = 32
EXPERTS = 32
CAP = 4
N_SP = 32
N_TP = 4


def draw_head_bias(key, part):
    return jax.random.uniform(key, (HEADS,), jnp.float32, -14.0, -5.0)


def shard_levels(own_key, dims, split, least, largest):
    gain, own = 1.0, jax.random.fold_in(own_key, 6)
    for axis_at, parts in split:
        steps = jnp.exp(jax.random.uniform(jax.random.fold_in(own, axis_at), (parts,), jnp.float32, least / len(split), largest / len(split)))
        gain = gain * jnp.repeat(steps, dims[axis_at] // parts).reshape([-1 if axis == axis_at else 1 for axis in range(len(dims))])
    return gain


def split_up(amount, total, reach, lean):
    loads = [(1 << 20) // math.isqrt(rank ** lean) + 1 for rank in range(2, amount + 1)]
    spare, holding = total - reach - (amount - 1), [1] * (amount - 1)
    while spare > 0:
        free = [i for i in range(amount - 1) if holding[i] < reach]
        whole, remaining = sum([loads[i] for i in free]), spare
        for i in free:
            extra = min(reach - holding[i], max(1, remaining * loads[i] // whole), spare)
            holding[i] = holding[i] + extra
            spare = spare - extra
    return np.array([reach] + holding)


def ragged_sizes(rng, count, total, reach, slope):
    if count == 2:
        one = jax.random.randint(rng, (), max(1, total - reach), min(reach, total - 1) + 1)
        return jnp.stack([one, total - one])
    sizes = jnp.asarray(split_up(count, total, reach, slope), jnp.int32)
    couples = (count - 1) // 2
    giver, taker = sizes[1:1 + 2 * couples:2], sizes[2:2 + 2 * couples:2]
    slack = jnp.minimum(giver - 1, reach - taker)
    shifted = jax.random.randint(jax.random.fold_in(rng, 1), (couples,), 0, 1 << 20) % (slack + 1)
    sizes = sizes.at[1:1 + 2 * couples:2].set(giver - shifted).at[2:2 + 2 * couples:2].set(taker + shifted)
    return sizes[jax.random.permutation(jax.random.fold_in(rng, 2), count)]


def assign_block(own_key, own, number, rows, number_of, top, most, slope):
    order = jax.random.permutation(own_key, number_of)
    packed, common = shares(number_of, rows * top, most, slope, True), shares(number_of, rows * top, most, slope, False)
    places = jnp.arange(number_of)

    def named(tallies, offset_by):
        used = int((tallies > 0).sum())
        fixed = max(1, used // 4)
        shifted = fixed + (places - fixed + offset_by * (used - fixed)) % max(1, number_of - fixed)
        return jnp.zeros((number_of,), jnp.int32).at[order[jnp.where(places < fixed, places, shifted)]].set(jnp.asarray(tallies, jnp.int32))

    tallies = jnp.where(number % 4 == 0, named(packed, number // 4), named(common, number - number // 4 - 1))
    mixed = jax.random.permutation(jax.random.fold_in(own, 3), number_of)
    donor, taker = mixed[0:number_of // 2 * 2:2], mixed[1:number_of // 2 * 2:2]
    room = jnp.minimum(tallies[donor] - 1, most - tallies[taker]) // 2
    room = jnp.where((donor == order[0]) | (taker == order[0]) | (tallies[taker] == 0), 0, jnp.maximum(room, 0))
    shifted = jax.random.randint(jax.random.fold_in(own, 4), (number_of // 2,), 0, 1 << 20) % (room + 1)
    tallies = tallies.at[donor].add(-shifted).at[taker].add(shifted)
    labels = jnp.searchsorted(jnp.cumsum(tallies), jnp.arange(rows * top), side="right").astype(jnp.int32)
    table = labels.reshape(top, rows).T
    table = table[jax.random.permutation(jax.random.fold_in(own, 1), rows)]
    offset_by = jax.random.randint(jax.random.fold_in(own, 2), (rows, 1), 0, top)
    return jnp.take_along_axis(table, (jnp.arange(top)[None, :] + offset_by) % top, axis=1)


def shares(amount, total, reach, skew, full):
    loads = [(1 << 20) // math.isqrt(grade ** skew) + 1 for grade in range(1, amount + 1)]
    largest = reach if full else min(reach, max(-(-total // amount), total * loads[0] // sum(loads)))
    least = 1 if total - largest >= amount - 1 else 0
    given, rest = [largest] + [least] * (amount - 1), total - largest - least * (amount - 1)
    while rest > 0:
        candidates = [i for i in range(1, amount) if given[i] < largest] or [i for i in range(1, amount) if given[i] < reach]
        whole, budget = sum([loads[i] for i in candidates]), rest
        for i in candidates:
            extra = min(reach - given[i], max(1, budget * loads[i] // whole), rest)
            given[i] = given[i] + extra
            rest = rest - extra
    return np.array(given)


def centred(own_key, shape, width, most, split=(), kind=jnp.bfloat16):
    result = jax.random.normal(own_key, shape, jnp.float32) * width
    if len(split) > 0:
        result = shard_levels(own_key, shape, split, -0.22, 0.18) * result
    return jnp.clip(result, min=-most, max=most).astype(kind)


def setup_inputs(seed: int = 0, part: int = 0) -> dict:
    key_list = jax.random.split(jax.random.key(seed), 14)
    own_keys = jax.random.split(jax.random.fold_in(key_list[13], part), 14)
    queries = centred(own_keys[0], (SEQ, HEADS * DH), 2.0, 8.0, ((0, 32), (1, 4)))
    keys = centred(own_keys[1], (SEQ, KV_HEADS * DH), 1.0, 6.0, ((0, 32), (1, 4)))
    values = centred(own_keys[2], (SEQ, KV_HEADS * DH), 1.0, 6.0, ((0, 32), (1, 4)))
    head_bias = draw_head_bias(jax.random.fold_in(key_list[13], 71), part)
    documents = jnp.searchsorted(jnp.cumsum(ragged_sizes(own_keys[4], DOCS, SEQ, 3 * SEQ // 4, 0)), jnp.arange(SEQ), side="right").astype(jnp.int32)
    w_out = centred(key_list[5], (HEADS * DH, D), (HEADS * DH) ** -0.5, 0.125, ((0, 4),))
    resid = centred(own_keys[6], (SEQ, D), 1.0, 6.0, ((0, 128),))
    norm_gain = jnp.clip(1.0 + 0.18 * jax.random.normal(key_list[7], (D,), jnp.float32), 0.1, 1.9)
    expert_ids_keys = jax.random.split(jax.random.fold_in(own_keys[8], 1), SEQ // ROWS)
    expert_ids_turns = jax.random.permutation(jax.random.fold_in(own_keys[8], 3), SEQ // ROWS)
    expert_ids = jax.vmap(lambda own, number: assign_block(jax.random.fold_in(own_keys[8], 2), own, number, ROWS, EXPERTS, TOPK, CAP, 1))(expert_ids_keys, expert_ids_turns).reshape((SEQ, TOPK))
    expert_gates = jnp.clip(0.1 + 0.79999997 * jax.random.uniform(own_keys[9], (SEQ, TOPK), jnp.float32) ** shard_levels(own_keys[9], (SEQ, TOPK), ((0, 128),), -0.2, 0.2), 0.1, 0.9)
    w_gate = centred(key_list[10], (EXPERTS, D, FF), D ** -0.5, 0.125, ((0, 32), (2, 4)))
    w_up = centred(key_list[11], (EXPERTS, D, FF), D ** -0.5, 0.125, ((0, 32), (2, 4)))
    w_down = centred(key_list[12], (EXPERTS, FF, D), FF ** -0.5, 0.109375, ((0, 32), (1, 4)))
    return {"queries": queries, "keys": keys, "values": values, "head_bias": head_bias, "documents": documents, "w_out": w_out, "resid": resid, "norm_gain": norm_gain, "expert_ids": expert_ids, "expert_gates": expert_gates, "w_gate": w_gate, "w_up": w_up, "w_down": w_down}


def rounded(array):
    return lax.optimization_barrier(array.astype(jnp.bfloat16)).astype(jnp.float32)

def reference(queries, keys, values, head_bias, documents, w_out, resid, norm_gain, expert_ids, expert_gates, w_gate, w_up, w_down):
    highest = lax.Precision.HIGHEST
    group_size = HEADS // KV_HEADS
    scale_factor = DH ** (-0.5)
    query_all = queries.astype(jnp.float32).reshape(SEQ, KV_HEADS, group_size, DH)
    key_all = keys.astype(jnp.float32).reshape(SEQ, KV_HEADS, DH)
    value_all = values.astype(jnp.float32).reshape(SEQ, KV_HEADS, DH)
    bias_grid = head_bias.astype(jnp.float32).reshape(KV_HEADS, group_size)
    positions = jnp.arange(SEQ, dtype=jnp.int32)
    block_rows = math.gcd(SEQ, 256)

    def attend_block(block_index):
        first = block_index * block_rows
        query_block = lax.dynamic_slice_in_dim(query_all, first, block_rows, 0)
        query_pos = first + jnp.arange(block_rows, dtype=jnp.int32)
        query_doc = lax.dynamic_slice_in_dim(documents, first, block_rows, 0)
        live = (positions[None, :] < query_pos[:, None]) & (documents[None, :] == query_doc[:, None])
        logits = jnp.einsum('qgrd,sgd->grqs', query_block, key_all, precision=highest) * scale_factor + bias_grid[:, :, None, None]
        keep = jnp.where(live, jax.nn.log_sigmoid(-logits), 0.0)
        after = lax.cumsum(keep, axis=3, reverse=True) - keep
        weight = rounded(jnp.where(live, jnp.exp(jax.nn.log_sigmoid(logits) + after), 0.0))
        mixed_block = jnp.einsum('grqs,sgd->qgrd', weight, value_all, precision=highest)
        return mixed_block.reshape(block_rows, HEADS * DH).astype(jnp.bfloat16)
    mixed = lax.map(attend_block, jnp.arange(SEQ // block_rows, dtype=jnp.int32)).reshape(SEQ, HEADS * DH)
    share = HEADS * DH // N_TP
    partials = jnp.einsum('sjc,jcd->sjd', mixed.astype(jnp.float32).reshape(SEQ, N_TP, share), w_out.astype(jnp.float32).reshape(N_TP, share, D), precision=highest)
    middle = (resid.astype(jnp.float32) + lax.optimization_barrier(jnp.sum(rounded(partials), axis=1))).astype(jnp.bfloat16)
    middle_value = middle.astype(jnp.float32)
    normed = (middle_value * lax.rsqrt(lax.optimization_barrier(jnp.mean(middle_value * middle_value, axis=1, keepdims=True)) + 1e-06) * norm_gain.astype(jnp.float32)).astype(jnp.bfloat16)
    assignments = SEQ * TOPK
    most_rows = N_SP * N_TP * CAP
    flat_ids = expert_ids.reshape(-1)
    hidden_share = FF // N_TP

    def run_expert(expert):
        picks = jnp.nonzero(flat_ids == expert, size=most_rows, fill_value=assignments)[0].astype(jnp.int32)
        source = normed[jnp.minimum(picks, assignments - 1) // TOPK].astype(jnp.float32)
        gate_value = jnp.dot(source, w_gate[expert].astype(jnp.float32), precision=highest)
        up_value = jnp.dot(source, w_up[expert].astype(jnp.float32), precision=highest)
        hidden = rounded(jax.nn.silu(gate_value) * up_value).reshape(most_rows, N_TP, hidden_share)
        partial_out = jnp.einsum('bjf,jfd->bjd', hidden, w_down[expert].astype(jnp.float32).reshape(N_TP, hidden_share, D), precision=highest)
        return (lax.optimization_barrier(jnp.sum(rounded(partial_out), axis=1)).astype(jnp.bfloat16), picks)
    outputs, picks_all = lax.map(run_expert, jnp.arange(EXPERTS, dtype=jnp.int32))
    routed = jnp.zeros((assignments, D), jnp.bfloat16).at[picks_all.reshape(-1)].set(outputs.reshape(-1, D), mode='drop')
    combined = lax.optimization_barrier(jnp.sum(expert_gates.astype(jnp.float32)[:, :, None] * routed.reshape(SEQ, TOPK, D).astype(jnp.float32), axis=1))
    return (middle_value + combined).astype(jnp.bfloat16)
```

```python
import functools
import math

import jax
import jax.numpy as jnp
from jax import lax
from jax.experimental import pallas as pl
from jax.experimental.pallas import tpu as pltpu
from jax.sharding import PartitionSpec as P

D = 2048
HEADS = 16
KV_HEADS = 8
DH = 128
TOPK = 2
SP = "sp"
GRP_SP = ("grp", "sp")
GRP_SP_TP = ("grp", "sp", "tp")


def sent_together(arrays, axis, dim, along):
    widths = [a.shape[along] for a in arrays]
    both = jnp.concatenate(arrays, axis=along)
    filled = lax.all_gather(both, axis, axis=dim, tiled=True)
    return tuple(jnp.split(filled, [sum(widths[:k]) for k in range(1, len(widths))], axis=along))


def in_blocks(shard, dim, peers):
    before, after = (shard.shape[:dim], shard.shape[dim + 1 :])
    return jnp.moveaxis(shard.reshape(*before, peers, -1, *after), dim, 0)


def summed_on_arrival(shard, axis, dim):
    blocks = in_blocks(shard, dim, lax.axis_size(axis))
    arrived = lax.all_to_all(blocks, axis, split_axis=0, concat_axis=0, tiled=True)
    return arrived.astype(jnp.float32).sum(axis=0)


def laid_out(blocks, dim):
    blocks = jnp.moveaxis(blocks, 0, dim)
    shape = blocks.shape
    return blocks.reshape(*shape[:dim], shape[dim] * shape[dim + 1], *shape[dim + 2 :])


def turned_blocks(blocks, axes, sequence):
    shape = [lax.axis_size(a) for a in axes]
    blocks = blocks.reshape(*shape, *blocks.shape[1:])
    for k in sequence:
        blocks = lax.all_to_all(blocks, axes[k], split_axis=k, concat_axis=k, tiled=True)
    return blocks.reshape(-1, *blocks.shape[len(axes) :])


def core_and_chips(shard, groups, sequence, split_dim, concat_dim):
    peers = lax.axis_size(groups[0]) * lax.axis_size(groups[1])
    blocks = in_blocks(shard, split_dim, peers)
    return laid_out(turned_blocks(blocks, groups, sequence), concat_dim)


def from_everyone(shard, axis):
    copies = jnp.broadcast_to(shard, (lax.axis_size(axis), *shard.shape))
    return lax.all_to_all(copies, axis, split_axis=0, concat_axis=0, tiled=True)


def collect(shard, axis, dim):
    blocks = from_everyone(shard, axis)
    return laid_out(blocks, dim)


MESH_ID = pl.DeviceIdType.MESH
LOG2E = math.log2(math.e)


def remote(src, dst, send, recv, axis, index):
    return pltpu.make_async_remote_copy(
        src_ref=src,
        dst_ref=dst,
        send_sem=send,
        recv_sem=recv,
        device_id={axis: index},
        device_id_type=MESH_ID,
    )


def attention_kernel(
    chips,
    reach,
    q_ref,
    k_ref,
    v_ref,
    doc_row_ref,
    doc_col_ref,
    bias_ref,
    out_ref,
    kv,
    qx,
    doc_col,
    tri,
    near,
    far,
    carry,
    mix,
    mixed_in,
    pair_send,
    pair_recv,
    own_sem,
    up_send,
    up_recv,
    down_send,
    down_recv,
    back_send,
    back_recv,
):
    tok = q_ref.shape[0]
    both = 2 * tok
    me = lax.axis_index("sp")
    chip = me // 2
    core = me % 2
    other = 1 - core
    partner = chip * 2 + other
    up = lax.rem(chip + 1, chips) * 2 + core
    down = lax.rem(chip + chips - 1, chips) * 2 + core
    up_steps = chips // 2
    down_steps = chips - 1 - up_steps

    barrier = pltpu.get_barrier_semaphore()
    for peer in (partner, up, down):
        pl.semaphore_signal(barrier, inc=1, device_id={"sp": peer}, device_id_type=MESH_ID)

    def at(x, size=None):
        return pl.ds(pl.multiple_of(x, 128), size or tok)

    doc_rows = doc_row_ref.shape[0]
    rows_here = at(core * tok)
    moves = []
    for h in range(2):
        moves.append((lambda o, h=h: q_ref.at[:, at(o * 256 + h * 128, 128)], qx.at[at(h * both + core * tok), :]))
    moves.append((lambda o: k_ref.at[:, at(o * 128, 128)], kv.at[chip, rows_here, :]))
    moves.append((lambda o: v_ref.at[:, at(o * 128, 128)], kv.at[chip, at(both + core * tok), :]))
    moves.append(
        (
            lambda o: doc_row_ref,
            kv.at[chip, pl.ds(pl.multiple_of(2 * both + core * doc_rows, doc_rows), doc_rows), :],
        )
    )
    moves.append((lambda o: doc_col_ref, doc_col.at[rows_here, :]))
    kept = [pltpu.make_async_copy(src(core), dst, own_sem.at[i]) for i, (src, dst) in enumerate(moves)]
    for copy in kept:
        copy.start()
    pl.semaphore_wait(barrier, 3)
    traded = [
        remote(src(other), dst, pair_send.at[i], pair_recv.at[i], "sp", partner)
        for i, (src, dst) in enumerate(moves)
    ]
    for i in (2, 3, 4, 0, 1, 5):
        traded[i].start()
    row_id = lax.broadcasted_iota(jnp.int32, (both, both), 0)
    col_id = lax.broadcasted_iota(jnp.int32, (both, both), 1)
    tri[...] = (row_id > col_id).astype(jnp.bfloat16)
    near[...] = jnp.zeros_like(near)
    far[...] = jnp.zeros_like(far)
    carry[...] = jnp.zeros_like(carry)

    pieces = ((0, both), (both, both + 2 * doc_rows))

    def upward(step, piece):
        block = lax.rem(chip - step + chips, chips)
        first, count = pieces[piece]
        ref = kv.at[block, pl.ds(first, count), :]
        return remote(ref, ref, up_send.at[step, piece], up_recv.at[step, piece], "sp", up)

    def downward(step, piece):
        block = lax.rem(chip + step, chips)
        first, count = pieces[piece]
        ref = kv.at[block, pl.ds(first, count), :]
        return remote(ref, ref, down_send.at[step, piece], down_recv.at[step, piece], "sp", down)

    def arrived_up(step, piece):
        block = lax.rem(chip - step - 1 + chips, chips)
        first, count = pieces[piece]
        ref = kv.at[block, pl.ds(first, count), :]
        return remote(ref, ref, up_send.at[step, piece], up_recv.at[step, piece], "sp", up)

    def arrived_down(step, piece):
        block = lax.rem(chip + step + 1, chips)
        first, count = pieces[piece]
        ref = kv.at[block, pl.ds(first, count), :]
        return remote(ref, ref, down_send.at[step, piece], down_recv.at[step, piece], "sp", down)

    for i in (2, 3, 4):
        kept[i].wait()
    traded[2].wait_recv()
    upward(0, 0).start()
    downward(0, 0).start()
    traded[3].wait_recv()
    traded[4].wait_recv()
    upward(0, 1).start()
    downward(0, 1).start()
    for i in (0, 1, 5):
        kept[i].wait()
        traded[i].wait_recv()

    scale = LOG2E / math.sqrt(128.0)

    def piece_of(block, i, diagonal):
        rows = pl.ds(i * tok, tok)
        head, first = i // 2, (i % 2) * tok
        logits = lax.dot_general(
            qx[rows, :],
            kv[block, 0:both, :],
            (((1,), (1,)), ((), ())),
            preferred_element_type=jnp.float32,
        )
        logits = logits * scale + bias_ref[2 * core + head] * LOG2E
        tail = jnp.log(1.0 + jnp.exp2(-jnp.abs(logits))) * LOG2E
        spend = jnp.maximum(logits, 0.0) + tail
        gain = jnp.minimum(logits, 0.0) - tail
        doc_here = doc_col[pl.ds(first, tok), :].astype(jnp.float32)
        doc_here = jnp.concatenate([doc_here, doc_here], axis=1)
        low = kv[block, 2 * both : 2 * both + doc_rows, :].astype(jnp.float32)
        high = kv[block, 2 * both + doc_rows : 2 * both + 2 * doc_rows, :].astype(jnp.float32)
        doc_there = jnp.concatenate([low[0:1], high[0:1]], axis=1)
        live = doc_here == doc_there
        if diagonal:
            t = first + lax.broadcasted_iota(jnp.int32, (tok, both), 0)
            s = lax.broadcasted_iota(jnp.int32, (tok, both), 1)
            live = live & (s < t)
            spend = jnp.where(live, spend, 0.0)
        coarse = spend.astype(jnp.bfloat16)
        fine = (spend - coarse.astype(jnp.float32)).astype(jnp.bfloat16)
        later = jnp.dot(coarse, tri[...], preferred_element_type=jnp.float32) + jnp.dot(
            fine, tri[...], preferred_element_type=jnp.float32
        )
        weight = jnp.where(live, jnp.exp2(gain - later), 0.0).astype(jnp.bfloat16)
        share = jnp.dot(weight, kv[block, both : 2 * both, :], preferred_element_type=jnp.float32)
        whole = jnp.broadcast_to(later[:, 0:1] + spend[:, 0:1], (tok, 128))
        return rows, share, whole

    for i in range(4):
        rows, share, whole = piece_of(chip, i, True)
        near[rows, :] = share
        carry[rows, :] = whole

    def visit(step, _):
        for piece in range(2):
            arrived_up(step, piece).wait_recv()

            @pl.when(step + 1 < up_steps)
            def _():
                upward(step + 1, piece).start()

            @pl.when(step < down_steps)
            def _():
                arrived_down(step, piece).wait_recv()

                @pl.when(step + 1 < down_steps)
                def _():
                    downward(step + 1, piece).start()

        @pl.when(chip - step - 1 >= 0)
        def _():
            for i in range(4):
                rows, share, whole = piece_of(chip - step - 1, i, False)
                near[rows, :] += jnp.exp2(-carry[rows, :]) * share
                carry[rows, :] += whole

        wrapped = chip + step + 1 - chips

        @pl.when((step < down_steps) & (wrapped >= 0) & (chip - wrapped <= reach))
        def _():
            for i in range(4):
                rows, share, whole = piece_of(wrapped, i, False)
                far[rows, :] = jnp.exp2(-whole) * far[rows, :] + share

        return 0

    lax.fori_loop(0, up_steps, visit, 0)

    for h in range(2):
        rows = pl.ds(h * both, both)
        mix[h] = (near[rows, :] + jnp.exp2(-carry[rows, :]) * far[rows, :]).astype(jnp.bfloat16)
    back = [
        remote(
            mix.at[h, at(other * tok), :],
            mixed_in.at[h],
            back_send.at[h],
            back_recv.at[h],
            "sp",
            partner,
        )
        for h in range(2)
    ]
    for copy in back:
        copy.start()
    for h in range(2):
        out_ref[:, at(core * 256 + h * 128, 128)] = mix[h, at(core * tok), :]
    for h in range(2):
        back[h].wait_recv()
        out_ref[:, at(other * 256 + h * 128, 128)] = mixed_in[h]
    for copy in traded + back:
        copy.wait_send()

    def drain(step, _):
        for piece in range(2):
            upward(step, piece).wait_send()

            @pl.when(step < down_steps)
            def _():
                downward(step, piece).wait_send()

        return 0

    lax.fori_loop(0, up_steps, drain, 0)


def attention(queries, keys, values, head_bias, documents, chips):
    tok = queries.shape[0]
    both = 2 * tok
    doc = documents.astype(jnp.bfloat16)
    doc_rows = 16
    doc_row = jnp.broadcast_to(doc[None, :], (doc_rows, tok))
    doc_col = jnp.broadcast_to(doc[:, None], (tok, 128))
    longest = chips * both * 3 // 4
    reach = (longest - 1 + both - 1) // both
    up_steps = chips // 2
    vmem = pl.BlockSpec(memory_space=pltpu.VMEM)
    dma = pltpu.SemaphoreType.DMA
    return pl.pallas_call(
        functools.partial(attention_kernel, chips, reach),
        out_shape=jax.ShapeDtypeStruct((tok, 512), jnp.bfloat16),
        in_specs=[vmem] * 5 + [pl.BlockSpec(memory_space=pltpu.SMEM)],
        out_specs=vmem,
        scratch_shapes=[
            pltpu.VMEM((chips, 2 * both + 2 * doc_rows, 128), jnp.bfloat16),
            pltpu.VMEM((2 * both, 128), jnp.bfloat16),
            pltpu.VMEM((both, 128), jnp.bfloat16),
            pltpu.VMEM((both, both), jnp.bfloat16),
            pltpu.VMEM((2 * both, 128), jnp.float32),
            pltpu.VMEM((2 * both, 128), jnp.float32),
            pltpu.VMEM((2 * both, 128), jnp.float32),
            pltpu.VMEM((2, both, 128), jnp.bfloat16),
            pltpu.VMEM((2, tok, 128), jnp.bfloat16),
            dma((6,)),
            dma((6,)),
            dma((6,)),
            dma((up_steps, 2)),
            dma((up_steps, 2)),
            dma((up_steps, 2)),
            dma((up_steps, 2)),
            dma((2,)),
            dma((2,)),
        ],
        compiler_params=pltpu.CompilerParams(collective_id=0, has_side_effects=True),
        name="attention",
    )(queries, keys, values, doc_row, doc_col, head_bias)


def local(
    queries,
    keys,
    values,
    head_bias,
    documents,
    w_out,
    resid,
    norm_gain,
    expert_ids,
    expert_gates,
    w_gate,
    w_up,
    w_down,
):
    sp_count = lax.axis_size("sp")
    tp_count = lax.axis_size("tp")
    mixed = attention(queries, keys, values, head_bias, documents, sp_count // 2)
    projected = summed_on_arrival(
        jnp.dot(mixed, w_out, preferred_element_type=jnp.float32).astype(jnp.bfloat16), "tp", 0
    )
    middle = (resid.astype(jnp.float32) + projected).astype(jnp.bfloat16)
    middle_value = middle.astype(jnp.float32)
    normed = (
        middle_value
        * lax.rsqrt(jnp.mean(middle_value * middle_value, axis=1, keepdims=True) + 1e-06)
        * norm_gain
    ).astype(jnp.bfloat16)
    row_count = normed.shape[0]
    expert_count = w_gate.shape[0] * sp_count
    slot_limit = min(row_count, max(2, 2 * TOPK * row_count // expert_count))
    flat_ids = expert_ids.reshape(-1)
    onehot_ids = (flat_ids[:, None] == jnp.arange(expert_count, dtype=jnp.int32)[None, :]).astype(
        jnp.int32
    )
    earlier = jnp.cumsum(onehot_ids, axis=0) - onehot_ids
    slot_ids = jnp.sum(earlier * onehot_ids, axis=1)
    target = flat_ids * slot_limit + slot_ids
    placing = (
        jnp.arange(expert_count * slot_limit, dtype=jnp.int32)[:, None] == target[None, :]
    ).astype(jnp.bfloat16)
    by_token = jnp.sum(placing.reshape(expert_count * slot_limit, row_count, TOPK), axis=2)
    outgoing = jnp.dot(by_token, normed, preferred_element_type=jnp.float32).astype(jnp.bfloat16)
    outgoing = outgoing.reshape(expert_count, slot_limit, D)
    arrived = lax.all_to_all(outgoing, "sp", split_axis=0, concat_axis=0, tiled=True)
    gathered = collect(arrived, "tp", 0)
    expert_rows = gathered.reshape(-1, D)
    gate_value = jnp.dot(expert_rows, w_gate[0], preferred_element_type=jnp.float32)
    up_value = jnp.dot(expert_rows, w_up[0], preferred_element_type=jnp.float32)
    hidden = (jax.nn.silu(gate_value) * up_value).astype(jnp.bfloat16)
    partial_out = jnp.dot(hidden, w_down[0], preferred_element_type=jnp.float32)
    summed = summed_on_arrival(
        partial_out.reshape(tp_count, sp_count * slot_limit, D).astype(jnp.bfloat16), "tp", 0
    )
    expert_result = summed.reshape(sp_count, slot_limit, D).astype(jnp.bfloat16)
    returned = lax.all_to_all(expert_result, "sp", split_axis=0, concat_axis=0, tiled=True)
    routed = jnp.dot(placing.T, returned.reshape(-1, D), preferred_element_type=jnp.float32)
    combined = jnp.sum(expert_gates[:, :, None] * routed.reshape(row_count, TOPK, D), axis=1)
    return (middle_value + combined).astype(jnp.bfloat16)


def solution(mesh):
    in_specs = (
        P(GRP_SP, "tp"),
        P(GRP_SP, "tp"),
        P(GRP_SP, "tp"),
        P("tp"),
        P(GRP_SP),
        P("tp", None),
        P(GRP_SP_TP, None),
        P(),
        P(GRP_SP_TP, None),
        P(GRP_SP_TP, None),
        P(SP, None, "tp"),
        P(SP, None, "tp"),
        P(SP, "tp", None),
    )
    out_specs = P(GRP_SP_TP, None)
    return jax.shard_map(local, mesh=mesh, in_specs=in_specs, out_specs=out_specs, check_vma=False)
```

```python
import functools
import math

import jax
import jax.numpy as jnp
from jax import lax
from jax.experimental import pallas as pl
from jax.experimental.pallas import tpu as pltpu
from jax.sharding import PartitionSpec as P

TOPK = 2
SP = "sp"
GRP_SP = ("grp", "sp")
GRP_SP_TP = ("grp", "sp", "tp")


MESH_ID = pl.DeviceIdType.MESH
LOG2E = math.log2(math.e)


def remote(src, dst, send, recv, axis, index):
    return pltpu.make_async_remote_copy(
        src_ref=src,
        dst_ref=dst,
        send_sem=send,
        recv_sem=recv,
        device_id={axis: index},
        device_id_type=MESH_ID,
    )


def attention_kernel(
    chips,
    reach,
    q_ref,
    k_ref,
    v_ref,
    doc_row_ref,
    doc_col_ref,
    bias_ref,
    out_ref,
    kv,
    qx,
    doc_col,
    tri,
    near,
    far,
    carry,
    mix,
    mixed_in,
    pair_send,
    pair_recv,
    own_sem,
    up_send,
    up_recv,
    down_send,
    down_recv,
    back_send,
    back_recv,
):
    tok = q_ref.shape[0]
    both = 2 * tok
    me = lax.axis_index("sp")
    chip = me // 2
    core = me % 2
    other = 1 - core
    partner = chip * 2 + other
    up = lax.rem(chip + 1, chips) * 2 + core
    down = lax.rem(chip + chips - 1, chips) * 2 + core
    up_steps = chips // 2
    down_steps = chips - 1 - up_steps

    barrier = pltpu.get_barrier_semaphore()
    for peer in (partner, up, down):
        pl.semaphore_signal(barrier, inc=1, device_id={"sp": peer}, device_id_type=MESH_ID)

    def at(x, size=None):
        return pl.ds(pl.multiple_of(x, 128), size or tok)

    doc_rows = doc_row_ref.shape[0]
    rows_here = at(core * tok)
    moves = []
    for h in range(2):
        moves.append((lambda o, h=h: q_ref.at[:, at(o * 256 + h * 128, 128)], qx.at[at(h * both + core * tok), :]))
    moves.append((lambda o: k_ref.at[:, at(o * 128, 128)], kv.at[chip, rows_here, :]))
    moves.append((lambda o: v_ref.at[:, at(o * 128, 128)], kv.at[chip, at(both + core * tok), :]))
    moves.append(
        (
            lambda o: doc_row_ref,
            kv.at[chip, pl.ds(pl.multiple_of(2 * both + core * doc_rows, doc_rows), doc_rows), :],
        )
    )
    moves.append((lambda o: doc_col_ref, doc_col.at[rows_here, :]))
    kept = [pltpu.make_async_copy(src(core), dst, own_sem.at[i]) for i, (src, dst) in enumerate(moves)]
    for copy in kept:
        copy.start()
    pl.semaphore_wait(barrier, 3)
    traded = [
        remote(src(other), dst, pair_send.at[i], pair_recv.at[i], "sp", partner)
        for i, (src, dst) in enumerate(moves)
    ]
    for i in (2, 3, 4, 0, 1, 5):
        traded[i].start()
    row_id = lax.broadcasted_iota(jnp.int32, (both, both), 0)
    col_id = lax.broadcasted_iota(jnp.int32, (both, both), 1)
    tri[...] = (row_id > col_id).astype(jnp.bfloat16)
    near[...] = jnp.zeros_like(near)
    far[...] = jnp.zeros_like(far)
    carry[...] = jnp.zeros_like(carry)

    pieces = ((0, both), (both, both + 2 * doc_rows))

    def upward(step, piece):
        block = lax.rem(chip - step + chips, chips)
        first, count = pieces[piece]
        ref = kv.at[block, pl.ds(first, count), :]
        return remote(ref, ref, up_send.at[step, piece], up_recv.at[step, piece], "sp", up)

    def downward(step, piece):
        block = lax.rem(chip + step, chips)
        first, count = pieces[piece]
        ref = kv.at[block, pl.ds(first, count), :]
        return remote(ref, ref, down_send.at[step, piece], down_recv.at[step, piece], "sp", down)

    def arrived_up(step, piece):
        block = lax.rem(chip - step - 1 + chips, chips)
        first, count = pieces[piece]
        ref = kv.at[block, pl.ds(first, count), :]
        return remote(ref, ref, up_send.at[step, piece], up_recv.at[step, piece], "sp", up)

    def arrived_down(step, piece):
        block = lax.rem(chip + step + 1, chips)
        first, count = pieces[piece]
        ref = kv.at[block, pl.ds(first, count), :]
        return remote(ref, ref, down_send.at[step, piece], down_recv.at[step, piece], "sp", down)

    for i in (2, 3, 4):
        kept[i].wait()
    traded[2].wait_recv()
    upward(0, 0).start()
    downward(0, 0).start()
    traded[3].wait_recv()
    traded[4].wait_recv()
    upward(0, 1).start()
    downward(0, 1).start()
    for i in (0, 1, 5):
        kept[i].wait()
        traded[i].wait_recv()

    scale = LOG2E / math.sqrt(128.0)

    def piece_of(block, i, diagonal):
        rows = pl.ds(i * tok, tok)
        head, first = i // 2, (i % 2) * tok
        logits = lax.dot_general(
            qx[rows, :],
            kv[block, 0:both, :],
            (((1,), (1,)), ((), ())),
            preferred_element_type=jnp.float32,
        )
        logits = logits * scale + bias_ref[2 * core + head] * LOG2E
        tail = jnp.log(1.0 + jnp.exp2(-jnp.abs(logits))) * LOG2E
        spend = jnp.maximum(logits, 0.0) + tail
        gain = jnp.minimum(logits, 0.0) - tail
        doc_here = doc_col[pl.ds(first, tok), :].astype(jnp.float32)
        doc_here = jnp.concatenate([doc_here, doc_here], axis=1)
        low = kv[block, 2 * both : 2 * both + doc_rows, :].astype(jnp.float32)
        high = kv[block, 2 * both + doc_rows : 2 * both + 2 * doc_rows, :].astype(jnp.float32)
        doc_there = jnp.concatenate([low[0:1], high[0:1]], axis=1)
        live = doc_here == doc_there
        if diagonal:
            t = first + lax.broadcasted_iota(jnp.int32, (tok, both), 0)
            s = lax.broadcasted_iota(jnp.int32, (tok, both), 1)
            live = live & (s < t)
            spend = jnp.where(live, spend, 0.0)
        coarse = spend.astype(jnp.bfloat16)
        fine = (spend - coarse.astype(jnp.float32)).astype(jnp.bfloat16)
        later = jnp.dot(coarse, tri[...], preferred_element_type=jnp.float32) + jnp.dot(
            fine, tri[...], preferred_element_type=jnp.float32
        )
        weight = jnp.where(live, jnp.exp2(gain - later), 0.0).astype(jnp.bfloat16)
        share = jnp.dot(weight, kv[block, both : 2 * both, :], preferred_element_type=jnp.float32)
        whole = jnp.broadcast_to(later[:, 0:1] + spend[:, 0:1], (tok, 128))
        return rows, share, whole

    for i in range(4):
        rows, share, whole = piece_of(chip, i, True)
        near[rows, :] = share
        carry[rows, :] = whole

    def visit(step, _):
        for piece in range(2):
            arrived_up(step, piece).wait_recv()

            @pl.when(step + 1 < up_steps)
            def _():
                upward(step + 1, piece).start()

            @pl.when(step < down_steps)
            def _():
                arrived_down(step, piece).wait_recv()

                @pl.when(step + 1 < down_steps)
                def _():
                    downward(step + 1, piece).start()

        @pl.when(chip - step - 1 >= 0)
        def _():
            for i in range(4):
                rows, share, whole = piece_of(chip - step - 1, i, False)
                near[rows, :] += jnp.exp2(-carry[rows, :]) * share
                carry[rows, :] += whole

        wrapped = chip + step + 1 - chips

        @pl.when((step < down_steps) & (wrapped >= 0) & (chip - wrapped <= reach))
        def _():
            for i in range(4):
                rows, share, whole = piece_of(wrapped, i, False)
                far[rows, :] = jnp.exp2(-whole) * far[rows, :] + share

        return 0

    lax.fori_loop(0, up_steps, visit, 0)

    for h in range(2):
        rows = pl.ds(h * both, both)
        mix[h] = (near[rows, :] + jnp.exp2(-carry[rows, :]) * far[rows, :]).astype(jnp.bfloat16)
    back = [
        remote(
            mix.at[h, at(other * tok), :],
            mixed_in.at[h],
            back_send.at[h],
            back_recv.at[h],
            "sp",
            partner,
        )
        for h in range(2)
    ]
    for copy in back:
        copy.start()
    for h in range(2):
        out_ref[:, at(core * 256 + h * 128, 128)] = mix[h, at(core * tok), :]
    for h in range(2):
        back[h].wait_recv()
        out_ref[:, at(other * 256 + h * 128, 128)] = mixed_in[h]
    for copy in traded + back:
        copy.wait_send()

    def drain(step, _):
        for piece in range(2):
            upward(step, piece).wait_send()

            @pl.when(step < down_steps)
            def _():
                downward(step, piece).wait_send()

        return 0

    lax.fori_loop(0, up_steps, drain, 0)


def attention(queries, keys, values, head_bias, documents, chips):
    tok = queries.shape[0]
    both = 2 * tok
    doc = documents.astype(jnp.bfloat16)
    doc_rows = 16
    doc_row = jnp.broadcast_to(doc[None, :], (doc_rows, tok))
    doc_col = jnp.broadcast_to(doc[:, None], (tok, 128))
    longest = chips * both * 3 // 4
    reach = (longest - 1 + both - 1) // both
    up_steps = chips // 2
    vmem = pl.BlockSpec(memory_space=pltpu.VMEM)
    dma = pltpu.SemaphoreType.DMA
    return pl.pallas_call(
        functools.partial(attention_kernel, chips, reach),
        out_shape=jax.ShapeDtypeStruct((tok, 512), jnp.bfloat16),
        in_specs=[vmem] * 5 + [pl.BlockSpec(memory_space=pltpu.SMEM)],
        out_specs=vmem,
        scratch_shapes=[
            pltpu.VMEM((chips, 2 * both + 2 * doc_rows, 128), jnp.bfloat16),
            pltpu.VMEM((2 * both, 128), jnp.bfloat16),
            pltpu.VMEM((both, 128), jnp.bfloat16),
            pltpu.VMEM((both, both), jnp.bfloat16),
            pltpu.VMEM((2 * both, 128), jnp.float32),
            pltpu.VMEM((2 * both, 128), jnp.float32),
            pltpu.VMEM((2 * both, 128), jnp.float32),
            pltpu.VMEM((2, both, 128), jnp.bfloat16),
            pltpu.VMEM((2, tok, 128), jnp.bfloat16),
            dma((6,)),
            dma((6,)),
            dma((6,)),
            dma((up_steps, 2)),
            dma((up_steps, 2)),
            dma((up_steps, 2)),
            dma((up_steps, 2)),
            dma((2,)),
            dma((2,)),
        ],
        compiler_params=pltpu.CompilerParams(collective_id=0, has_side_effects=True),
        name="attention",
    )(queries, keys, values, doc_row, doc_col, head_bias)


def feed_kernel(
    chips,
    mixed_ref,
    w_out_ref,
    resid_ref,
    gain_ref,
    slot_row_ref,
    slot_col_ref,
    gate_col_ref,
    w_gate_hbm,
    w_up_hbm,
    w_down_hbm,
    out_ref,
    w_gate,
    w_up,
    w_down,
    partial,
    first_a,
    first_b,
    summed,
    second_a,
    second_b,
    middle,
    stack,
    outgoing,
    inbox,
    rows_in,
    reply,
    returned,
    order,
    spread,
    weigh,
    weight_sem,
    self_sem,
    z_send,
    z_recv,
    a_send,
    a_recv,
    b_send,
    b_recv,
    relay_send,
    relay_recv,
    first_send,
    first_recv,
    second_send,
    second_recv,
    reply_send,
    reply_recv,
):
    waves = chips // 4
    half_ring = chips // 2
    peers = 2 * chips
    rows, width = resid_ref.shape
    quarter = width // 4
    half = width // 2
    me = lax.axis_index("sp")
    tp = lax.axis_index("tp")
    chip = me // 2
    core = me % 2
    low = tp % 2
    peer_a = tp + 1 - 2 * low
    peer_b = 3 - tp
    across = lax.rem(tp + 2, 4)

    loads = [
        pltpu.make_async_copy(src.at[0], dst, weight_sem.at[i])
        for i, (src, dst) in enumerate(((w_gate_hbm, w_gate), (w_up_hbm, w_up), (w_down_hbm, w_down)))
    ]
    for copy in loads:
        copy.start()

    barrier = pltpu.get_barrier_semaphore()

    def greet(k, _):
        pl.semaphore_signal(
            barrier, inc=1, device_id={"sp": lax.rem(me + k, peers)}, device_id_type=MESH_ID
        )
        return 0

    lax.fori_loop(1, peers, greet, 0)
    for peer in (peer_a, peer_b):
        pl.semaphore_signal(barrier, inc=1, device_id={"tp": peer}, device_id_type=MESH_ID)

    def block(n, which, first=0, size=None):
        return partial.at[n, pl.ds(pl.multiple_of(which * rows, rows), rows), pl.ds(first, size or width)]

    def first_send_of(n, i):
        owner = (peer_a, peer_b, across, across)[i]
        into = (first_a, first_b)[i % 2].at[n, i // 2]
        return remote(
            block(n, owner, (i % 2) * half, half),
            into,
            first_send.at[n, i],
            first_recv.at[n, i],
            "tp",
            (peer_a, peer_b)[i % 2],
        )

    def second_send_of(n, i):
        into = (second_b, second_a)[i].at[n]
        return remote(
            summed.at[n, i], into, second_send.at[n, i], second_recv.at[n, i], "tp", (peer_b, peer_a)[i]
        )

    def sum_start(n):
        for i in (2, 3, 0, 1):
            first_send_of(n, i).start()

    def sum_middle(n):
        first_send_of(n, 2).wait_recv()
        summed[n, 0] = (
            block(n, peer_b, 0, half)[...].astype(jnp.float32) + first_a[n, 1].astype(jnp.float32)
        ).astype(jnp.bfloat16)
        second_send_of(n, 0).start()
        first_send_of(n, 3).wait_recv()
        summed[n, 1] = (
            block(n, peer_a, half, half)[...].astype(jnp.float32) + first_b[n, 1].astype(jnp.float32)
        ).astype(jnp.bfloat16)
        second_send_of(n, 1).start()

    def sum_end(n):
        first_send_of(n, 0).wait_recv()
        first_send_of(n, 1).wait_recv()
        left = block(n, tp, 0, half)[...].astype(jnp.float32) + first_a[n, 0].astype(jnp.float32)
        right = block(n, tp, half, half)[...].astype(jnp.float32) + first_b[n, 0].astype(jnp.float32)
        second_send_of(n, 0).wait_recv()
        left = left + second_b[n].astype(jnp.float32)
        second_send_of(n, 1).wait_recv()
        right = right + second_a[n].astype(jnp.float32)
        return left, right

    for j in range(4):
        columns = pl.ds(j * quarter, quarter)
        partial[waves, :, columns] = jnp.dot(
            mixed_ref[...], w_out_ref[:, columns], preferred_element_type=jnp.float32
        ).astype(jnp.bfloat16)
    pl.semaphore_wait(barrier, peers - 1 + 2)
    sum_start(waves)

    r = lax.broadcasted_iota(jnp.int32, (128, 128), 0)
    c = lax.broadcasted_iota(jnp.int32, (128, 128), 1)
    order[0] = (((r & 31) >> 2) * 16 + (r >> 5) * 4 + (r & 3) == c).astype(jnp.bfloat16)
    order[1] = (((c & 31) >> 2) * 16 + (c >> 5) * 4 + (c & 3) == r).astype(jnp.bfloat16)
    tall = peers * 16
    r = lax.broadcasted_iota(jnp.int32, (tall, 128), 0)
    c = lax.broadcasted_iota(jnp.int32, (tall, 128), 1)
    place = (r >> 4) * 4 + (r & 3)
    hit = (place == slot_row_ref[0:1, :]) | (place == slot_row_ref[1:2, :])
    spread[...] = (hit & (((r >> 2) & 3) == (c >> 5))).astype(jnp.bfloat16)
    r = lax.broadcasted_iota(jnp.int32, (128, tall), 0)
    c = lax.broadcasted_iota(jnp.int32, (128, tall), 1)
    place = (c >> 4) * 4 + (c & 3)
    same = ((c >> 2) & 3) == (r >> 5)
    share = jnp.where(same & (place == slot_col_ref[:, 0:1]), gate_col_ref[:, 0:1], 0.0) + jnp.where(
        same & (place == slot_col_ref[:, 1:2]), gate_col_ref[:, 1:2], 0.0
    )
    coarse = share.astype(jnp.bfloat16)
    weigh[0] = coarse
    weigh[1] = (share - coarse.astype(jnp.float32)).astype(jnp.bfloat16)

    sum_middle(waves)
    left, right = sum_end(waves)
    for first, part in ((0, left), (half, right)):
        columns = pl.ds(first, half)
        middle[:, columns] = (resid_ref[:, columns].astype(jnp.float32) + part).astype(jnp.bfloat16)
    value = middle[...].astype(jnp.float32)
    value = value * lax.rsqrt(jnp.mean(value * value, axis=1, keepdims=True) + 1e-06) * gain_ref[...]
    value = value.astype(jnp.bfloat16)
    for j in range(4):
        stack[pl.ds(j * rows, rows), :] = value[:, j * quarter : (j + 1) * quarter]
    outgoing[...] = jnp.dot(spread[...], stack[...], preferred_element_type=jnp.float32).astype(jnp.bfloat16)

    def offsets(w):
        last = w == waves - 1
        far, close = half_ring - 1 - w, 1 + w
        return (far, -far, jnp.where(last, half_ring, close), jnp.where(last, 0, -close))

    def tile(x):
        return pl.ds(pl.multiple_of(x * 16, 16), 16)

    def dispatch(w, m, rel):
        target = lax.rem(chip - offsets(w)[m] + 2 * chips, chips) * 2 + lax.rem(core + rel, 2)
        return remote(
            outgoing.at[tile(target), :],
            inbox.at[w, tp, pl.ds((2 * m + rel) * 16, 16), :],
            z_send,
            z_recv.at[w, m // 2],
            "sp",
            target,
        )

    def answer(w, m, rel):
        target = lax.rem(chip + offsets(w)[m] + chips, chips) * 2 + lax.rem(core + rel, 2)
        return remote(
            reply.at[w, pl.ds((2 * m + rel) * 16, 16), :],
            returned.at[tile(me), :],
            reply_send,
            reply_recv,
            "sp",
            target,
        )

    def all_of(w, make):
        for m in range(4):
            for rel in range(2):
                if m == 3 and rel == 0:

                    @pl.when(w < waves - 1)
                    def _():
                        make(w, m, rel).start()

                else:
                    make(w, m, rel).start()

    own_in = pltpu.make_async_copy(
        outgoing.at[tile(me), :], inbox.at[waves - 1, tp, pl.ds(96, 16), :], self_sem.at[0]
    )
    own_out = pltpu.make_async_copy(
        reply.at[waves - 1, pl.ds(96, 16), :], returned.at[tile(me), :], self_sem.at[1]
    )
    own_in.start()

    def send_all(w, _):
        all_of(w, dispatch)
        return 0

    lax.fori_loop(0, waves, send_all, 0)

    def part(w, owner, h):
        return inbox.at[w, owner, pl.ds(h * 64, 64), :]

    def to_a(w, h, owner):
        return remote(part(w, owner, h), part(w, owner, h), a_send.at[w, h], a_recv.at[w, h], "tp", peer_a)

    def to_b(w, h, owner):
        return remote(part(w, owner, h), part(w, owner, h), b_send.at[w, h], b_recv.at[w, h], "tp", peer_b)

    def relay_a(w, owner):
        return remote(part(w, owner, 0), part(w, owner, 0), relay_send.at[w, 0], relay_recv.at[w, 0], "tp", peer_a)

    def relay_b(w, owner):
        return remote(part(w, owner, 1), part(w, owner, 1), relay_send.at[w, 1], relay_recv.at[w, 1], "tp", peer_b)

    def landed(w, h, count):
        ref = inbox.at[w, tp, pl.ds(h * 64, count), :]
        return remote(ref, ref, z_send, z_recv.at[w, h], "sp", lax.rem(me + 1, peers))

    def forward(w):
        landed(w, 0, 64).wait_recv()
        to_a(w, 0, tp).start()
        to_b(w, 0, tp).start()

        @pl.when(w < waves - 1)
        def _():
            landed(w, 1, 64).wait_recv()

        @pl.when(w == waves - 1)
        def _():
            landed(w, 1, 48).wait_recv()
            own_in.wait()

        to_a(w, 1, tp).start()
        to_b(w, 1, tp).start()

    def pass_on(w):
        to_b(w, 0, peer_b).wait_recv()
        relay_a(w, peer_b).start()
        to_a(w, 1, peer_a).wait_recv()
        relay_b(w, peer_a).start()

    def compute(w):
        to_a(w, 0, peer_a).wait_recv()
        to_b(w, 1, peer_b).wait_recv()
        relay_a(w, across).wait_recv()
        relay_b(w, across).wait_recv()
        for j in range(4):
            turned = jnp.dot(order[0], inbox[w, j], preferred_element_type=jnp.float32).astype(jnp.bfloat16)
            for k in range(4):
                rows_in[pl.ds(j * 32, 32), pl.ds(k * quarter, quarter)] = turned[k * 32 : (k + 1) * 32]
        gate = jnp.dot(rows_in[...], w_gate[...], preferred_element_type=jnp.float32)
        lift = jnp.dot(rows_in[...], w_up[...], preferred_element_type=jnp.float32)
        hidden = (gate / (1.0 + jnp.exp(-gate)) * lift).astype(jnp.bfloat16)
        for j in range(4):
            columns = pl.ds(j * quarter, quarter)
            partial[w, :, columns] = jnp.dot(
                hidden, w_down[:, columns], preferred_element_type=jnp.float32
            ).astype(jnp.bfloat16)
        sum_start(w)

    def give_back(w):
        left, right = sum_end(w)
        left, right = left.astype(jnp.bfloat16), right.astype(jnp.bfloat16)
        whole = jnp.concatenate(
            [left[:, :quarter], left[:, quarter:], right[:, :quarter], right[:, quarter:]], axis=0
        )
        reply[w] = jnp.dot(order[1], whole, preferred_element_type=jnp.float32).astype(jnp.bfloat16)
        all_of(w, answer)

        @pl.when(w == waves - 1)
        def _():
            own_out.start()

    for copy in loads:
        copy.wait()

    def turn(it, _):
        @pl.when(it < waves)
        def _():
            forward(it)

        @pl.when((it >= 2) & (it < waves + 2))
        def _():
            sum_middle(it - 2)

        @pl.when((it >= 1) & (it < waves + 1))
        def _():
            compute(it - 1)

        @pl.when(it < waves)
        def _():
            pass_on(it)

        @pl.when((it >= 2) & (it < waves + 2))
        def _():
            give_back(it - 2)

        return 0

    lax.fori_loop(0, waves + 2, turn, 0)

    rest = (peers - 1) * 16
    own_out.wait()
    everything = returned.at[pl.ds(0, rest), :]
    remote(everything, everything, reply_send, reply_recv, "sp", lax.rem(me + 1, peers)).wait_recv()
    mixed_rows = jnp.dot(weigh[0], returned[...], preferred_element_type=jnp.float32) + jnp.dot(
        weigh[1], returned[...], preferred_element_type=jnp.float32
    )
    for j in range(4):
        columns = pl.ds(j * quarter, quarter)
        out_ref[:, columns] = (
            middle[:, columns].astype(jnp.float32) + mixed_rows[j * rows : (j + 1) * rows]
        ).astype(jnp.bfloat16)

    sent = outgoing.at[pl.ds(0, rest), :]
    remote(sent, sent, z_send, z_recv.at[0, 0], "sp", lax.rem(me + 1, peers)).wait_send()
    remote(everything, everything, reply_send, reply_recv, "sp", lax.rem(me + 1, peers)).wait_send()

    def drain(w, _):
        for i in range(4):
            first_send_of(w, i).wait_send()
        for i in range(2):
            second_send_of(w, i).wait_send()

        @pl.when(w < waves)
        def _():
            for h in range(2):
                to_a(w, h, tp).wait_send()
                to_b(w, h, tp).wait_send()
            relay_a(w, peer_b).wait_send()
            relay_b(w, peer_a).wait_send()

        return 0

    lax.fori_loop(0, waves + 1, drain, 0)


def feed(mixed, w_out, resid, norm_gain, expert_ids, expert_gates, w_gate, w_up, w_down, chips):
    rows, width = resid.shape
    quarter, half = width // 4, width // 2
    peers = 2 * chips
    waves = chips // 4
    hidden = w_gate.shape[2]
    flat = expert_ids.reshape(-1)
    index = jnp.arange(flat.shape[0], dtype=jnp.int32)
    rank = jnp.sum(
        ((flat[:, None] == flat[None, :]) & (index[None, :] < index[:, None])).astype(jnp.int32), axis=1
    )
    slot = (flat * 4 + rank).reshape(rows, TOPK)
    slot_col = jnp.tile(slot, (4, 1))
    slot_row = slot_col.T
    gate_col = jnp.tile(expert_gates, (4, 1))
    vmem = pl.BlockSpec(memory_space=pltpu.VMEM)
    hbm = pl.BlockSpec(memory_space=pl.ANY)
    dma = pltpu.SemaphoreType.DMA
    bf16 = jnp.bfloat16
    return pl.pallas_call(
        functools.partial(feed_kernel, chips),
        out_shape=jax.ShapeDtypeStruct((rows, width), bf16),
        in_specs=[vmem] * 7 + [hbm] * 3,
        out_specs=vmem,
        scratch_shapes=[
            pltpu.VMEM((width, hidden), bf16),
            pltpu.VMEM((width, hidden), bf16),
            pltpu.VMEM((hidden, width), bf16),
            pltpu.VMEM((waves + 1, 4 * rows, width), bf16),
            pltpu.VMEM((waves + 1, 2, rows, half), bf16),
            pltpu.VMEM((waves + 1, 2, rows, half), bf16),
            pltpu.VMEM((waves + 1, 2, rows, half), bf16),
            pltpu.VMEM((waves + 1, rows, half), bf16),
            pltpu.VMEM((waves + 1, rows, half), bf16),
            pltpu.VMEM((rows, width), bf16),
            pltpu.VMEM((4 * rows, quarter), bf16),
            pltpu.VMEM((peers * 16, quarter), bf16),
            pltpu.VMEM((waves, 4, 128, quarter), bf16),
            pltpu.VMEM((128, width), bf16),
            pltpu.VMEM((waves, 128, quarter), bf16),
            pltpu.VMEM((peers * 16, quarter), bf16),
            pltpu.VMEM((2, 128, 128), bf16),
            pltpu.VMEM((peers * 16, 128), bf16),
            pltpu.VMEM((2, 128, peers * 16), bf16),
            dma((3,)),
            dma((2,)),
            dma,
            dma((waves, 2)),
            dma((waves, 2)),
            dma((waves, 2)),
            dma((waves, 2)),
            dma((waves, 2)),
            dma((waves, 2)),
            dma((waves, 2)),
            dma((waves + 1, 4)),
            dma((waves + 1, 4)),
            dma((waves + 1, 2)),
            dma((waves + 1, 2)),
            dma,
            dma,
        ],
        compiler_params=pltpu.CompilerParams(
            collective_id=1, has_side_effects=True, vmem_limit_bytes=48 * 1024 * 1024
        ),
        name="feed",
    )(mixed, w_out, resid, norm_gain.reshape(1, -1), slot_row, slot_col, gate_col, w_gate, w_up, w_down)


def local(
    queries,
    keys,
    values,
    head_bias,
    documents,
    w_out,
    resid,
    norm_gain,
    expert_ids,
    expert_gates,
    w_gate,
    w_up,
    w_down,
):
    chips = lax.axis_size("sp") // 2
    mixed = attention(queries, keys, values, head_bias, documents, chips)
    return feed(
        mixed, w_out, resid, norm_gain, expert_ids, expert_gates, w_gate, w_up, w_down, chips
    )


def solution(mesh):
    in_specs = (
        P(GRP_SP, "tp"),
        P(GRP_SP, "tp"),
        P(GRP_SP, "tp"),
        P("tp"),
        P(GRP_SP),
        P("tp", None),
        P(GRP_SP_TP, None),
        P(),
        P(GRP_SP_TP, None),
        P(GRP_SP_TP, None),
        P(SP, None, "tp"),
        P(SP, None, "tp"),
        P(SP, "tp", None),
    )
    out_specs = P(GRP_SP_TP, None)
    return jax.shard_map(local, mesh=mesh, in_specs=in_specs, out_specs=out_specs, check_vma=False)
```

```python
import functools
import math

import jax
import jax.numpy as jnp
from jax import lax
from jax.experimental import pallas as pl
from jax.experimental.pallas import tpu as pltpu
from jax.sharding import PartitionSpec as P

MESH_ID = pl.DeviceIdType.MESH
LOG2E = math.log2(math.e)


def remote(src, dst, send, recv, axis, index):
    return pltpu.make_async_remote_copy(
        src_ref=src,
        dst_ref=dst,
        send_sem=send,
        recv_sem=recv,
        device_id={axis: index},
        device_id_type=MESH_ID,
    )


def layer_kernel(
    chips,
    reach,
    q_ref,
    k_ref,
    v_ref,
    w_out_hbm,
    resid_hbm,
    w_gate_hbm,
    w_up_hbm,
    w_down_hbm,
    doc_ref,
    gain_ref,
    ids_ref,
    gates_ref,
    bias_ref,
    out_ref,
    kv,
    qx,
    doc_rows_own,
    doc_col,
    tri,
    near,
    far,
    carry,
    mix,
    mixed,
    pair_send,
    pair_recv,
    own_sem,
    up_send,
    up_recv,
    down_send,
    down_recv,
    back_send,
    back_recv,
    w_out,
    w_gate,
    w_up,
    w_down,
    resid,
    partial,
    first_a,
    first_b,
    summed,
    second_a,
    second_b,
    middle,
    stack,
    outgoing,
    inbox,
    rows_in,
    reply,
    returned,
    order,
    spread,
    weigh,
    lines,
    weight_sem,
    self_sem,
    z_send,
    z_recv,
    a_send,
    a_recv,
    b_send,
    b_recv,
    relay_send,
    relay_recv,
    first_send,
    first_recv,
    second_send,
    second_recv,
    reply_send,
    reply_recv,
):
    tok = q_ref.shape[0]
    both = 2 * tok
    me = lax.axis_index("sp")
    tp = lax.axis_index("tp")
    chip = me // 2
    core = me % 2
    other = 1 - core
    partner = chip * 2 + other
    up = lax.rem(chip + 1, chips) * 2 + core
    down = lax.rem(chip + chips - 1, chips) * 2 + core
    up_steps = chips // 2
    down_steps = chips - 1 - up_steps

    peer_a = tp + 1 - 2 * (tp % 2)
    peer_b = 3 - tp
    across = lax.rem(tp + 2, 4)

    barrier = pltpu.get_barrier_semaphore()
    for peer in (partner, up, down):
        pl.semaphore_signal(barrier, inc=1, device_id={"sp": peer}, device_id_type=MESH_ID)
    for peer in (peer_a, peer_b):
        pl.semaphore_signal(barrier, inc=1, device_id={"tp": peer}, device_id_type=MESH_ID)

    def at(x, size=None):
        return pl.ds(pl.multiple_of(x, 128), size or tok)

    doc_rows = doc_rows_own.shape[0]
    rows_here = at(core * tok)
    moves = [
        (lambda o: k_ref.at[:, at(o * 128, 128)], kv.at[chip, rows_here, :]),
        (lambda o: v_ref.at[:, at(o * 128, 128)], kv.at[chip, at(both + core * tok), :]),
        (
            lambda o: doc_rows_own,
            kv.at[chip, pl.ds(pl.multiple_of(2 * both + core * doc_rows, doc_rows), doc_rows), :],
        ),
    ]
    for h in range(2):
        moves.append((lambda o, h=h: q_ref.at[:, at(o * 256 + h * 128, 128)], qx.at[at(h * both + core * tok), :]))
    doc_rows_own[...] = jnp.broadcast_to(doc_ref[...].astype(jnp.float32), (doc_rows, tok)).astype(jnp.bfloat16)
    kept = [pltpu.make_async_copy(src(core), dst, own_sem.at[i]) for i, (src, dst) in enumerate(moves)]
    for copy in kept:
        copy.start()
    pl.semaphore_wait(barrier, 5)
    traded = [
        remote(src(other), dst, pair_send.at[i], pair_recv.at[i], "sp", partner)
        for i, (src, dst) in enumerate(moves)
    ]
    for copy in traded:
        copy.start()
    loads = [
        pltpu.make_async_copy(src, dst, weight_sem.at[i])
        for i, (src, dst) in enumerate(
            (
                (w_out_hbm, w_out),
                (resid_hbm, resid),
                (w_gate_hbm.at[0], w_gate),
                (w_up_hbm.at[0], w_up),
                (w_down_hbm.at[0], w_down),
            )
        )
    ]
    for copy in loads:
        copy.start()
    row_id = lax.broadcasted_iota(jnp.int32, (both, both), 0)
    col_id = lax.broadcasted_iota(jnp.int32, (both, both), 1)
    tri[...] = (row_id > col_id).astype(jnp.bfloat16)
    near[...] = jnp.zeros_like(near)
    far[...] = jnp.zeros_like(far)
    carry[...] = jnp.zeros_like(carry)

    peers = 2 * chips
    rows = resid.shape[0]
    r = lax.broadcasted_iota(jnp.int32, (128, 128), 0)
    c = lax.broadcasted_iota(jnp.int32, (128, 128), 1)
    order[0] = (((r & 31) >> 2) * 16 + (r >> 5) * 4 + (r & 3) == c).astype(jnp.bfloat16)
    order[1] = (((c & 31) >> 2) * 16 + (c >> 5) * 4 + (c & 3) == r).astype(jnp.bfloat16)
    lines[...] = jnp.zeros_like(lines)
    lines[0:2, 0:rows] = ids_ref[...].astype(jnp.float32)
    lines[2:4, 0:rows] = gates_ref[...]
    tiled = lines[...]
    tiled = tiled + pltpu.roll(tiled, rows, 1)
    tiled = tiled + pltpu.roll(tiled, 2 * rows, 1)
    first_there, second_there, first_gate, second_gate = (
        jnp.broadcast_to(tiled[k : k + 1], (128, 128)) for k in range(4)
    )
    first_here, second_here, first_gate, second_gate = (
        x.T for x in (first_there, second_there, first_gate, second_gate)
    )
    once = c < rows
    before = once & (c < (r & (rows - 1)))

    def count(found):
        return jnp.sum(found.astype(jnp.float32), axis=1, keepdims=True)

    first_slot = first_here[:, 0:1] * 4.0 + count(before & (first_here == first_there))
    second_slot = (
        second_here[:, 0:1] * 4.0
        + count(once & (second_here == first_there))
        + count(before & (second_here == second_there))
    )
    first_line = jnp.broadcast_to(first_slot, (128, 128)).T[0:1].astype(jnp.int32)
    second_line = jnp.broadcast_to(second_slot, (128, 128)).T[0:1].astype(jnp.int32)
    first_slot = first_slot.astype(jnp.int32)
    second_slot = second_slot.astype(jnp.int32)
    tall = peers * 16
    r = lax.broadcasted_iota(jnp.int32, (tall, 128), 0)
    c = lax.broadcasted_iota(jnp.int32, (tall, 128), 1)
    place = (r >> 4) * 4 + (r & 3)
    hit = (place == first_line) | (place == second_line)
    spread[...] = (hit & (((r >> 2) & 3) == (c >> 5))).astype(jnp.bfloat16)
    r = lax.broadcasted_iota(jnp.int32, (128, tall), 0)
    c = lax.broadcasted_iota(jnp.int32, (128, tall), 1)
    place = (c >> 4) * 4 + (c & 3)
    same = ((c >> 2) & 3) == (r >> 5)
    share = jnp.where(same & (place == first_slot), first_gate[:, 0:1], 0.0) + jnp.where(
        same & (place == second_slot), second_gate[:, 0:1], 0.0
    )
    coarse = share.astype(jnp.bfloat16)
    weigh[0] = coarse
    weigh[1] = (share - coarse.astype(jnp.float32)).astype(jnp.bfloat16)


    pieces = ((0, both), (both, both + 2 * doc_rows))

    def upward(step, piece):
        block = lax.rem(chip - step + chips, chips)
        first, count = pieces[piece]
        ref = kv.at[block, pl.ds(first, count), :]
        return remote(ref, ref, up_send.at[step, piece], up_recv.at[step, piece], "sp", up)

    def downward(step, piece):
        block = lax.rem(chip + step, chips)
        first, count = pieces[piece]
        ref = kv.at[block, pl.ds(first, count), :]
        return remote(ref, ref, down_send.at[step, piece], down_recv.at[step, piece], "sp", down)

    def arrived_up(step, piece):
        block = lax.rem(chip - step - 1 + chips, chips)
        first, count = pieces[piece]
        ref = kv.at[block, pl.ds(first, count), :]
        return remote(ref, ref, up_send.at[step, piece], up_recv.at[step, piece], "sp", up)

    def arrived_down(step, piece):
        block = lax.rem(chip + step + 1, chips)
        first, count = pieces[piece]
        ref = kv.at[block, pl.ds(first, count), :]
        return remote(ref, ref, down_send.at[step, piece], down_recv.at[step, piece], "sp", down)

    kept[0].wait()
    traded[0].wait_recv()
    upward(0, 0).start()
    downward(0, 0).start()
    for i in (1, 2):
        kept[i].wait()
        traded[i].wait_recv()
    upward(0, 1).start()
    downward(0, 1).start()
    for i in (3, 4):
        kept[i].wait()
        traded[i].wait_recv()
    for i in range(2):
        line = kv[chip, 2 * both + i * doc_rows : 2 * both + (i + 1) * doc_rows, :].astype(jnp.float32)
        doc_col[i * tok : (i + 1) * tok, :] = jnp.broadcast_to(line[0:1], (tok, tok)).T

    scale = LOG2E / math.sqrt(128.0)

    def piece_of(block, i, diagonal):
        rows = pl.ds(i * tok, tok)
        head, first = i // 2, (i % 2) * tok
        logits = lax.dot_general(
            qx[rows, :],
            kv[block, 0:both, :],
            (((1,), (1,)), ((), ())),
            preferred_element_type=jnp.float32,
        )
        logits = logits * scale + bias_ref[2 * core + head] * LOG2E
        tail = jnp.log(1.0 + jnp.exp2(-jnp.abs(logits))) * LOG2E
        spend = jnp.maximum(logits, 0.0) + tail
        gain = jnp.minimum(logits, 0.0) - tail
        doc_here = doc_col[pl.ds(first, tok), :]
        doc_here = jnp.concatenate([doc_here, doc_here], axis=1)
        low = kv[block, 2 * both : 2 * both + doc_rows, :].astype(jnp.float32)
        high = kv[block, 2 * both + doc_rows : 2 * both + 2 * doc_rows, :].astype(jnp.float32)
        doc_there = jnp.concatenate([low[0:1], high[0:1]], axis=1)
        live = doc_here == doc_there
        if diagonal:
            t = first + lax.broadcasted_iota(jnp.int32, (tok, both), 0)
            s = lax.broadcasted_iota(jnp.int32, (tok, both), 1)
            live = live & (s < t)
            spend = jnp.where(live, spend, 0.0)
        coarse = spend.astype(jnp.bfloat16)
        fine = (spend - coarse.astype(jnp.float32)).astype(jnp.bfloat16)
        later = jnp.dot(coarse, tri[...], preferred_element_type=jnp.float32) + jnp.dot(
            fine, tri[...], preferred_element_type=jnp.float32
        )
        weight = jnp.where(live, jnp.exp2(gain - later), 0.0).astype(jnp.bfloat16)
        share = jnp.dot(weight, kv[block, both : 2 * both, :], preferred_element_type=jnp.float32)
        whole = jnp.broadcast_to(later[:, 0:1] + spend[:, 0:1], (tok, 128))
        return rows, share, whole

    for i in range(4):
        rows, share, whole = piece_of(chip, i, True)
        near[rows, :] = share
        carry[rows, :] = whole

    def visit(step, _):
        for piece in range(2):
            arrived_up(step, piece).wait_recv()

            @pl.when(step + 1 < up_steps)
            def _():
                upward(step + 1, piece).start()

            @pl.when(step < down_steps)
            def _():
                arrived_down(step, piece).wait_recv()

                @pl.when(step + 1 < down_steps)
                def _():
                    downward(step + 1, piece).start()

        @pl.when(chip - step - 1 >= 0)
        def _():
            for i in range(4):
                rows, share, whole = piece_of(chip - step - 1, i, False)
                near[rows, :] += jnp.exp2(-carry[rows, :]) * share
                carry[rows, :] += whole

        wrapped = chip + step + 1 - chips

        @pl.when((step < down_steps) & (wrapped >= 0) & (chip - wrapped <= reach))
        def _():
            for i in range(4):
                rows, share, whole = piece_of(wrapped, i, False)
                far[rows, :] = jnp.exp2(-whole) * far[rows, :] + share

        return 0

    lax.fori_loop(0, up_steps, visit, 0)

    for h in range(2):
        rows = pl.ds(h * both, both)
        mix[h] = (near[rows, :] + jnp.exp2(-carry[rows, :]) * far[rows, :]).astype(jnp.bfloat16)
    def mixed_at(h):
        return mixed.at[:, at(core * 256 + h * 128, 128)]

    back = [
        remote(mix.at[h, at(other * tok), :], mixed_at(h), back_send.at[h], back_recv.at[h], "sp", partner)
        for h in range(2)
    ]
    for copy in back:
        copy.start()
    for h in range(2):
        mixed[:, at(core * 256 + h * 128, 128)] = mix[h, at(core * tok), :]
    for copy in back:
        copy.wait_recv()

    waves = chips // 4
    half_ring = chips // 2
    peers = 2 * chips
    rows, width = resid.shape
    quarter = width // 4
    half = width // 2

    def block(n, which, first=0, size=None):
        return partial.at[n, pl.ds(pl.multiple_of(which * rows, rows), rows), pl.ds(first, size or width)]

    def first_send_of(n, i):
        owner = (peer_a, peer_b, across, across)[i]
        into = (first_a, first_b)[i % 2].at[n, i // 2]
        return remote(
            block(n, owner, (i % 2) * half, half),
            into,
            first_send.at[n, i],
            first_recv.at[n, i],
            "tp",
            (peer_a, peer_b)[i % 2],
        )

    def second_send_of(n, i):
        into = (second_b, second_a)[i].at[n]
        return remote(
            summed.at[n, i], into, second_send.at[n, i], second_recv.at[n, i], "tp", (peer_b, peer_a)[i]
        )

    def sum_start(n):
        for i in (2, 3, 0, 1):
            first_send_of(n, i).start()

    def sum_middle(n):
        first_send_of(n, 2).wait_recv()
        summed[n, 0] = (
            block(n, peer_b, 0, half)[...].astype(jnp.float32) + first_a[n, 1].astype(jnp.float32)
        ).astype(jnp.bfloat16)
        second_send_of(n, 0).start()
        first_send_of(n, 3).wait_recv()
        summed[n, 1] = (
            block(n, peer_a, half, half)[...].astype(jnp.float32) + first_b[n, 1].astype(jnp.float32)
        ).astype(jnp.bfloat16)
        second_send_of(n, 1).start()

    def sum_end(n):
        first_send_of(n, 0).wait_recv()
        first_send_of(n, 1).wait_recv()
        left = block(n, tp, 0, half)[...].astype(jnp.float32) + first_a[n, 0].astype(jnp.float32)
        right = block(n, tp, half, half)[...].astype(jnp.float32) + first_b[n, 0].astype(jnp.float32)
        second_send_of(n, 0).wait_recv()
        left = left + second_b[n].astype(jnp.float32)
        second_send_of(n, 1).wait_recv()
        right = right + second_a[n].astype(jnp.float32)
        return left, right

    for copy in loads:
        copy.wait()
    for j in range(4):
        columns = pl.ds(j * quarter, quarter)
        partial[waves, :, columns] = jnp.dot(
            mixed[...], w_out[:, columns], preferred_element_type=jnp.float32
        ).astype(jnp.bfloat16)
    sum_start(waves)

    sum_middle(waves)
    left, right = sum_end(waves)
    for first, part in ((0, left), (half, right)):
        columns = pl.ds(first, half)
        middle[:, columns] = (resid[:, columns].astype(jnp.float32) + part).astype(jnp.bfloat16)
    value = middle[...].astype(jnp.float32)
    value = value * lax.rsqrt(jnp.mean(value * value, axis=1, keepdims=True) + 1e-06) * gain_ref[...]
    value = value.astype(jnp.bfloat16)
    for j in range(4):
        stack[pl.ds(j * rows, rows), :] = value[:, j * quarter : (j + 1) * quarter]
    outgoing[...] = jnp.dot(spread[...], stack[...], preferred_element_type=jnp.float32).astype(jnp.bfloat16)

    def offsets(w):
        last = w == waves - 1
        far, close = half_ring - 1 - w, 1 + w
        return (far, -far, jnp.where(last, half_ring, close), jnp.where(last, 0, -close))

    def tile(x):
        return pl.ds(pl.multiple_of(x * 16, 16), 16)

    def dispatch(w, m, rel):
        target = lax.rem(chip - offsets(w)[m] + 2 * chips, chips) * 2 + lax.rem(core + rel, 2)
        return remote(
            outgoing.at[tile(target), :],
            inbox.at[w, tp, pl.ds((2 * m + rel) * 16, 16), :],
            z_send,
            z_recv.at[w, m // 2],
            "sp",
            target,
        )

    def answer(w, m, rel):
        target = lax.rem(chip + offsets(w)[m] + chips, chips) * 2 + lax.rem(core + rel, 2)
        return remote(
            reply.at[w, pl.ds((2 * m + rel) * 16, 16), :],
            returned.at[tile(me), :],
            reply_send,
            reply_recv,
            "sp",
            target,
        )

    def all_of(w, make):
        for m in range(4):
            for rel in range(2):
                if m == 3 and rel == 0:

                    @pl.when(w < waves - 1)
                    def _():
                        make(w, m, rel).start()

                else:
                    make(w, m, rel).start()

    own_in = pltpu.make_async_copy(
        outgoing.at[tile(me), :], inbox.at[waves - 1, tp, pl.ds(96, 16), :], self_sem.at[0]
    )
    own_out = pltpu.make_async_copy(
        reply.at[waves - 1, pl.ds(96, 16), :], returned.at[tile(me), :], self_sem.at[1]
    )
    own_in.start()

    def send_all(w, _):
        all_of(w, dispatch)
        return 0

    lax.fori_loop(0, waves, send_all, 0)

    def part(w, owner, h):
        return inbox.at[w, owner, pl.ds(h * 64, 64), :]

    def to_a(w, h, owner):
        return remote(part(w, owner, h), part(w, owner, h), a_send.at[w, h], a_recv.at[w, h], "tp", peer_a)

    def to_b(w, h, owner):
        return remote(part(w, owner, h), part(w, owner, h), b_send.at[w, h], b_recv.at[w, h], "tp", peer_b)

    def relay_a(w, owner):
        return remote(part(w, owner, 0), part(w, owner, 0), relay_send.at[w, 0], relay_recv.at[w, 0], "tp", peer_a)

    def relay_b(w, owner):
        return remote(part(w, owner, 1), part(w, owner, 1), relay_send.at[w, 1], relay_recv.at[w, 1], "tp", peer_b)

    def landed(w, h, count):
        ref = inbox.at[w, tp, pl.ds(h * 64, count), :]
        return remote(ref, ref, z_send, z_recv.at[w, h], "sp", lax.rem(me + 1, peers))

    def forward(w):
        landed(w, 0, 64).wait_recv()
        to_a(w, 0, tp).start()
        to_b(w, 0, tp).start()

        @pl.when(w < waves - 1)
        def _():
            landed(w, 1, 64).wait_recv()

        @pl.when(w == waves - 1)
        def _():
            landed(w, 1, 48).wait_recv()
            own_in.wait()

        to_a(w, 1, tp).start()
        to_b(w, 1, tp).start()

    def pass_on(w):
        to_b(w, 0, peer_b).wait_recv()
        relay_a(w, peer_b).start()
        to_a(w, 1, peer_a).wait_recv()
        relay_b(w, peer_a).start()

    def compute(w):
        to_a(w, 0, peer_a).wait_recv()
        to_b(w, 1, peer_b).wait_recv()
        relay_a(w, across).wait_recv()
        relay_b(w, across).wait_recv()
        for j in range(4):
            turned = jnp.dot(order[0], inbox[w, j], preferred_element_type=jnp.float32).astype(jnp.bfloat16)
            for k in range(4):
                rows_in[pl.ds(j * 32, 32), pl.ds(k * quarter, quarter)] = turned[k * 32 : (k + 1) * 32]
        gate = jnp.dot(rows_in[...], w_gate[...], preferred_element_type=jnp.float32)
        lift = jnp.dot(rows_in[...], w_up[...], preferred_element_type=jnp.float32)
        hidden = (gate / (1.0 + jnp.exp(-gate)) * lift).astype(jnp.bfloat16)
        for j in range(4):
            columns = pl.ds(j * quarter, quarter)
            partial[w, :, columns] = jnp.dot(
                hidden, w_down[:, columns], preferred_element_type=jnp.float32
            ).astype(jnp.bfloat16)
        sum_start(w)

    def give_back(w):
        left, right = sum_end(w)
        left, right = left.astype(jnp.bfloat16), right.astype(jnp.bfloat16)
        whole = jnp.concatenate(
            [left[:, :quarter], left[:, quarter:], right[:, :quarter], right[:, quarter:]], axis=0
        )
        reply[w] = jnp.dot(order[1], whole, preferred_element_type=jnp.float32).astype(jnp.bfloat16)
        all_of(w, answer)

        @pl.when(w == waves - 1)
        def _():
            own_out.start()

    def turn(it, _):
        @pl.when(it < waves)
        def _():
            forward(it)

        @pl.when((it >= 2) & (it < waves + 2))
        def _():
            sum_middle(it - 2)

        @pl.when((it >= 1) & (it < waves + 1))
        def _():
            compute(it - 1)

        @pl.when(it < waves)
        def _():
            pass_on(it)

        @pl.when((it >= 2) & (it < waves + 2))
        def _():
            give_back(it - 2)

        return 0

    lax.fori_loop(0, waves + 2, turn, 0)

    rest = (peers - 1) * 16
    own_out.wait()
    everything = returned.at[pl.ds(0, rest), :]
    remote(everything, everything, reply_send, reply_recv, "sp", lax.rem(me + 1, peers)).wait_recv()
    mixed_rows = jnp.dot(weigh[0], returned[...], preferred_element_type=jnp.float32) + jnp.dot(
        weigh[1], returned[...], preferred_element_type=jnp.float32
    )
    for j in range(4):
        columns = pl.ds(j * quarter, quarter)
        out_ref[:, columns] = (
            middle[:, columns].astype(jnp.float32) + mixed_rows[j * rows : (j + 1) * rows]
        ).astype(jnp.bfloat16)

    sent = outgoing.at[pl.ds(0, rest), :]
    remote(sent, sent, z_send, z_recv.at[0, 0], "sp", lax.rem(me + 1, peers)).wait_send()
    remote(everything, everything, reply_send, reply_recv, "sp", lax.rem(me + 1, peers)).wait_send()

    def drain(w, _):
        for i in range(4):
            first_send_of(w, i).wait_send()
        for i in range(2):
            second_send_of(w, i).wait_send()

        @pl.when(w < waves)
        def _():
            for h in range(2):
                to_a(w, h, tp).wait_send()
                to_b(w, h, tp).wait_send()
            relay_a(w, peer_b).wait_send()
            relay_b(w, peer_a).wait_send()

        return 0

    lax.fori_loop(0, waves + 1, drain, 0)
    for copy in traded + back:
        copy.wait_send()

    def drain_ring(step, _):
        for piece in range(2):
            upward(step, piece).wait_send()

            @pl.when(step < down_steps)
            def _():
                downward(step, piece).wait_send()

        return 0

    lax.fori_loop(0, up_steps, drain_ring, 0)


def layer(
    queries,
    keys,
    values,
    head_bias,
    documents,
    w_out,
    resid,
    norm_gain,
    expert_ids,
    expert_gates,
    w_gate,
    w_up,
    w_down,
):
    chips = lax.axis_size("sp") // 2
    tok = queries.shape[0]
    both = 2 * tok
    doc_rows = 16
    longest = chips * both * 3 // 4
    reach = (longest - 1 + both - 1) // both
    up_steps = chips // 2
    rows, width = resid.shape
    quarter, half = width // 4, width // 2
    peers = 2 * chips
    waves = chips // 4
    hidden = w_gate.shape[2]
    smem = pl.BlockSpec(memory_space=pltpu.SMEM)
    vmem = pl.BlockSpec(memory_space=pltpu.VMEM)
    hbm = pl.BlockSpec(memory_space=pl.ANY)
    dma = pltpu.SemaphoreType.DMA
    bf16, f32 = jnp.bfloat16, jnp.float32
    return pl.pallas_call(
        functools.partial(layer_kernel, chips, reach),
        out_shape=jax.ShapeDtypeStruct((rows, width), bf16),
        in_specs=[hbm] * 8 + [vmem] * 4 + [smem],
        out_specs=vmem,
        scratch_shapes=[
            pltpu.VMEM((chips, 2 * both + 2 * doc_rows, 128), bf16),
            pltpu.VMEM((2 * both, 128), bf16),
            pltpu.VMEM((doc_rows, tok), bf16),
            pltpu.VMEM((both, 128), f32),
            pltpu.VMEM((both, both), bf16),
            pltpu.VMEM((2 * both, 128), f32),
            pltpu.VMEM((2 * both, 128), f32),
            pltpu.VMEM((2 * both, 128), f32),
            pltpu.VMEM((2, both, 128), bf16),
            pltpu.VMEM((tok, 512), bf16),
            dma((5,)),
            dma((5,)),
            dma((5,)),
            dma((up_steps, 2)),
            dma((up_steps, 2)),
            dma((up_steps, 2)),
            dma((up_steps, 2)),
            dma((2,)),
            dma((2,)),
            pltpu.VMEM(w_out.shape, bf16),
            pltpu.VMEM((width, hidden), bf16),
            pltpu.VMEM((width, hidden), bf16),
            pltpu.VMEM((hidden, width), bf16),
            pltpu.VMEM((rows, width), bf16),
            pltpu.VMEM((waves + 1, 4 * rows, width), bf16),
            pltpu.VMEM((waves + 1, 2, rows, half), bf16),
            pltpu.VMEM((waves + 1, 2, rows, half), bf16),
            pltpu.VMEM((waves + 1, 2, rows, half), bf16),
            pltpu.VMEM((waves + 1, rows, half), bf16),
            pltpu.VMEM((waves + 1, rows, half), bf16),
            pltpu.VMEM((rows, width), bf16),
            pltpu.VMEM((4 * rows, quarter), bf16),
            pltpu.VMEM((peers * 16, quarter), bf16),
            pltpu.VMEM((waves, 4, 128, quarter), bf16),
            pltpu.VMEM((128, width), bf16),
            pltpu.VMEM((waves, 128, quarter), bf16),
            pltpu.VMEM((peers * 16, quarter), bf16),
            pltpu.VMEM((2, 128, 128), bf16),
            pltpu.VMEM((peers * 16, 128), bf16),
            pltpu.VMEM((2, 128, peers * 16), bf16),
            pltpu.VMEM((8, 128), f32),
            dma((5,)),
            dma((2,)),
            dma,
            dma((waves, 2)),
            dma((waves, 2)),
            dma((waves, 2)),
            dma((waves, 2)),
            dma((waves, 2)),
            dma((waves, 2)),
            dma((waves, 2)),
            dma((waves + 1, 4)),
            dma((waves + 1, 4)),
            dma((waves + 1, 2)),
            dma((waves + 1, 2)),
            dma,
            dma,
        ],
        compiler_params=pltpu.CompilerParams(collective_id=0, has_side_effects=True),
        name="layer",
    )(
        queries,
        keys,
        values,
        w_out,
        resid,
        w_gate,
        w_up,
        w_down,
        documents.reshape(1, -1),
        norm_gain.reshape(1, -1),
        expert_ids.T,
        expert_gates.T,
        head_bias,
    )


def solution(mesh):
    everyone = ("grp", "sp", "tp")
    in_specs = (
        P(("grp", "sp"), "tp"),
        P(("grp", "sp"), "tp"),
        P(("grp", "sp"), "tp"),
        P("tp"),
        P(("grp", "sp")),
        P("tp", None),
        P(everyone, None),
        P(),
        P(everyone, None),
        P(everyone, None),
        P("sp", None, "tp"),
        P("sp", None, "tp"),
        P("sp", "tp", None),
    )
    return jax.shard_map(layer, mesh=mesh, in_specs=in_specs, out_specs=P(everyone, None), check_vma=False)
```

```python
import functools
import math

import jax
import jax.numpy as jnp
from jax import lax
from jax.experimental import pallas as pl
from jax.experimental.pallas import tpu as pltpu
from jax.sharding import PartitionSpec as P

MESH_ID = pl.DeviceIdType.MESH
LOG2E = math.log2(math.e)


def remote(src, dst, send, recv, axis, index):
    return pltpu.make_async_remote_copy(
        src_ref=src,
        dst_ref=dst,
        send_sem=send,
        recv_sem=recv,
        device_id={axis: index},
        device_id_type=MESH_ID,
    )


def layer_kernel(
    chips,
    reach,
    q_ref,
    k_ref,
    v_ref,
    w_out_hbm,
    resid_hbm,
    w_gate_hbm,
    w_up_hbm,
    w_down_hbm,
    doc_ref,
    gain_ref,
    ids_ref,
    gates_ref,
    bias_ref,
    out_ref,
    kv,
    qx,
    doc_rows_own,
    doc_col,
    tri,
    near,
    far,
    carry,
    mix,
    mixed,
    known,
    pair_send,
    pair_recv,
    own_sem,
    up_send,
    up_recv,
    down_send,
    down_recv,
    back_send,
    back_recv,
    w_out,
    w_gate,
    w_up,
    w_down,
    resid,
    partial,
    first_a,
    first_b,
    summed,
    second_a,
    second_b,
    middle,
    stack,
    outgoing,
    inbox,
    rows_in,
    reply,
    returned,
    order,
    spread,
    weigh,
    lines,
    weight_sem,
    self_sem,
    z_send,
    z_recv,
    a_send,
    a_recv,
    b_send,
    b_recv,
    relay_send,
    relay_recv,
    first_send,
    first_recv,
    second_send,
    second_recv,
    reply_send,
    reply_recv,
):
    tok = q_ref.shape[0]
    both = 2 * tok
    me = lax.axis_index("sp")
    tp = lax.axis_index("tp")
    chip = me // 2
    core = me % 2
    other = 1 - core
    partner = chip * 2 + other
    up = lax.rem(chip + 1, chips) * 2 + core
    down = lax.rem(chip + chips - 1, chips) * 2 + core
    steps = chips // 2
    hi = steps - 2
    up_count = jnp.minimum(chip, steps)

    def need_up(c, b):
        return (c < chips) & (b >= c - steps)

    def need_down(c, b):
        return (b <= hi) & (b != c) & (lax.rem(b - c + chips, chips) < steps)

    def up_block(k):
        return chip - 1 - k

    def down_block(k):
        return lax.rem(chip + 1 + k, chips)

    def comes_down(k):
        return (k < steps - 1) & (down_block(k) <= hi)

    below = lax.rem(chip + chips - 1, chips)

    peer_a = tp + 1 - 2 * (tp % 2)
    peer_b = 3 - tp
    across = lax.rem(tp + 2, 4)

    barrier = pltpu.get_barrier_semaphore()
    for peer in (partner, up, down):
        pl.semaphore_signal(barrier, inc=1, device_id={"sp": peer}, device_id_type=MESH_ID)
    for peer in (peer_a, peer_b):
        pl.semaphore_signal(barrier, inc=1, device_id={"tp": peer}, device_id_type=MESH_ID)

    def at(x, size=None):
        return pl.ds(pl.multiple_of(x, 128), size or tok)

    doc_rows = doc_rows_own.shape[0]
    rows_here = at(core * tok)
    moves = [
        (lambda o: k_ref.at[:, at(o * 128, 128)], kv.at[chip, rows_here, :]),
        (lambda o: v_ref.at[:, at(o * 128, 128)], kv.at[chip, at(both + core * tok), :]),
        (
            lambda o: doc_rows_own,
            kv.at[chip, pl.ds(pl.multiple_of(2 * both + core * doc_rows, doc_rows), doc_rows), :],
        ),
    ]
    for h in range(2):
        moves.append((lambda o, h=h: q_ref.at[:, at(o * 256 + h * 128, 128)], qx.at[at(h * both + core * tok), :]))
    doc_rows_own[...] = jnp.broadcast_to(doc_ref[...].astype(jnp.float32), (doc_rows, tok)).astype(jnp.bfloat16)
    kept = [pltpu.make_async_copy(src(core), dst, own_sem.at[i]) for i, (src, dst) in enumerate(moves)]
    for copy in kept:
        copy.start()
    pl.semaphore_wait(barrier, 5)
    traded = [
        remote(src(other), dst, pair_send.at[i], pair_recv.at[i], "sp", partner)
        for i, (src, dst) in enumerate(moves)
    ]
    for copy in traded:
        copy.start()

    def tell(level):
        for step in (1 << level, chips - (1 << level)):
            pl.semaphore_signal(
                known.at[level],
                inc=1,
                device_id={"sp": lax.rem(chip + step, chips) * 2 + core},
                device_id_type=MESH_ID,
            )

    levels = (chips // 4).bit_length()
    tell(0)
    loads = [
        pltpu.make_async_copy(src, dst, weight_sem.at[i])
        for i, (src, dst) in enumerate(
            (
                (w_out_hbm, w_out),
                (resid_hbm, resid),
                (w_gate_hbm.at[0], w_gate),
                (w_up_hbm.at[0], w_up),
                (w_down_hbm.at[0], w_down),
            )
        )
    ]
    for copy in loads:
        copy.start()
    row_id = lax.broadcasted_iota(jnp.int32, (both, both), 0)
    col_id = lax.broadcasted_iota(jnp.int32, (both, both), 1)
    tri[...] = (row_id > col_id).astype(jnp.bfloat16)
    near[...] = jnp.zeros_like(near)
    far[...] = jnp.zeros_like(far)
    carry[...] = jnp.zeros_like(carry)

    peers = 2 * chips
    rows = resid.shape[0]
    r = lax.broadcasted_iota(jnp.int32, (128, 128), 0)
    c = lax.broadcasted_iota(jnp.int32, (128, 128), 1)
    order[0] = (((r & 31) >> 2) * 16 + (r >> 5) * 4 + (r & 3) == c).astype(jnp.bfloat16)
    order[1] = (((c & 31) >> 2) * 16 + (c >> 5) * 4 + (c & 3) == r).astype(jnp.bfloat16)
    lines[...] = jnp.zeros_like(lines)
    lines[0:2, 0:rows] = ids_ref[...].astype(jnp.float32)
    lines[2:4, 0:rows] = gates_ref[...]
    tiled = lines[...]
    tiled = tiled + pltpu.roll(tiled, rows, 1)
    tiled = tiled + pltpu.roll(tiled, 2 * rows, 1)
    first_there, second_there, first_gate, second_gate = (
        jnp.broadcast_to(tiled[k : k + 1], (128, 128)) for k in range(4)
    )
    first_here, second_here, first_gate, second_gate = (
        x.T for x in (first_there, second_there, first_gate, second_gate)
    )
    once = c < rows
    before = once & (c < (r & (rows - 1)))

    def tally(found):
        return jnp.sum(found.astype(jnp.float32), axis=1, keepdims=True)

    first_slot = first_here[:, 0:1] * 4.0 + tally(before & (first_here == first_there))
    second_slot = (
        second_here[:, 0:1] * 4.0
        + tally(once & (second_here == first_there))
        + tally(before & (second_here == second_there))
    )
    first_line = jnp.broadcast_to(first_slot, (128, 128)).T[0:1].astype(jnp.int32)
    second_line = jnp.broadcast_to(second_slot, (128, 128)).T[0:1].astype(jnp.int32)
    first_slot = first_slot.astype(jnp.int32)
    second_slot = second_slot.astype(jnp.int32)
    tall = peers * 16
    r = lax.broadcasted_iota(jnp.int32, (tall, 128), 0)
    c = lax.broadcasted_iota(jnp.int32, (tall, 128), 1)
    place = (r >> 4) * 4 + (r & 3)
    hit = (place == first_line) | (place == second_line)
    spread[...] = (hit & (((r >> 2) & 3) == (c >> 5))).astype(jnp.bfloat16)
    r = lax.broadcasted_iota(jnp.int32, (128, tall), 0)
    c = lax.broadcasted_iota(jnp.int32, (128, tall), 1)
    place = (c >> 4) * 4 + (c & 3)
    same = ((c >> 2) & 3) == (r >> 5)
    share = jnp.where(same & (place == first_slot), first_gate[:, 0:1], 0.0) + jnp.where(
        same & (place == second_slot), second_gate[:, 0:1], 0.0
    )
    coarse = share.astype(jnp.bfloat16)
    weigh[0] = coarse
    weigh[1] = (share - coarse.astype(jnp.float32)).astype(jnp.bfloat16)


    count = 2
    pieces = ((0, both), (both, both + 2 * doc_rows))

    def piece_ref(block, piece):
        return kv.at[block, pl.ds(*pieces[piece]), :]

    def upward(block, piece):
        ref = piece_ref(block, piece)
        return remote(ref, ref, up_send.at[block, piece], up_recv.at[block, piece], "sp", up)

    def downward(block, piece):
        ref = piece_ref(block, piece)
        return remote(ref, ref, down_send.at[block, piece], down_recv.at[block, piece], "sp", down)

    def send_on(block, piece):
        @pl.when(need_up(chip + 1, block))
        def _():
            upward(block, piece).start()

    def send_back(block, piece):
        @pl.when(need_down(below, block))
        def _():
            downward(block, piece).start()

    kept[0].wait()
    traded[0].wait_recv()
    for piece in range(count // 2):
        send_on(chip, piece)
        send_back(chip, piece)
    for i in (1, 2):
        kept[i].wait()
        traded[i].wait_recv()
    for piece in range(count // 2, count):
        send_on(chip, piece)
        send_back(chip, piece)
    for i in (3, 4):
        kept[i].wait()
        traded[i].wait_recv()
    for i in range(2):
        line = kv[chip, 2 * both + i * doc_rows : 2 * both + (i + 1) * doc_rows, :].astype(jnp.float32)
        doc_col[i * tok : (i + 1) * tok, :] = jnp.broadcast_to(line[0:1], (tok, tok)).T

    scale = LOG2E / math.sqrt(128.0)

    def piece_of(block, i, diagonal):
        rows = pl.ds(i * tok, tok)
        head, first = i // 2, (i % 2) * tok
        logits = lax.dot_general(
            qx[rows, :],
            kv[block, 0:both, :],
            (((1,), (1,)), ((), ())),
            preferred_element_type=jnp.float32,
        )
        logits = logits * scale + bias_ref[2 * core + head] * LOG2E
        tail = jnp.log(1.0 + jnp.exp2(-jnp.abs(logits))) * LOG2E
        spend = jnp.maximum(logits, 0.0) + tail
        gain = jnp.minimum(logits, 0.0) - tail
        doc_here = doc_col[pl.ds(first, tok), :]
        doc_here = jnp.concatenate([doc_here, doc_here], axis=1)
        low = kv[block, 2 * both : 2 * both + doc_rows, :].astype(jnp.float32)
        high = kv[block, 2 * both + doc_rows : 2 * both + 2 * doc_rows, :].astype(jnp.float32)
        doc_there = jnp.concatenate([low[0:1], high[0:1]], axis=1)
        live = doc_here == doc_there
        if diagonal:
            t = first + lax.broadcasted_iota(jnp.int32, (tok, both), 0)
            s = lax.broadcasted_iota(jnp.int32, (tok, both), 1)
            live = live & (s < t)
            spend = jnp.where(live, spend, 0.0)
        coarse = spend.astype(jnp.bfloat16)
        fine = (spend - coarse.astype(jnp.float32)).astype(jnp.bfloat16)
        later = jnp.dot(coarse, tri[...], preferred_element_type=jnp.float32) + jnp.dot(
            fine, tri[...], preferred_element_type=jnp.float32
        )
        weight = jnp.where(live, jnp.exp2(gain - later), 0.0).astype(jnp.bfloat16)
        share = jnp.dot(weight, kv[block, both : 2 * both, :], preferred_element_type=jnp.float32)
        whole = jnp.broadcast_to(later[:, 0:1] + spend[:, 0:1], (tok, 128))
        return rows, share, whole

    for i in range(4):
        rows, share, whole = piece_of(chip, i, True)
        near[rows, :] = share
        carry[rows, :] = whole

    def visit(k, _):
        for piece in range(count):

            @pl.when(k < up_count)
            def _():
                upward(up_block(k), piece).wait_recv()
                send_on(up_block(k), piece)

            @pl.when(comes_down(k))
            def _():
                downward(down_block(k), piece).wait_recv()
                send_back(down_block(k), piece)

        @pl.when(k < up_count)
        def _():
            for i in range(4):
                rows, share, whole = piece_of(up_block(k), i, False)
                near[rows, :] += jnp.exp2(-carry[rows, :]) * share
                carry[rows, :] += whole

        wrapped = down_block(k)

        @pl.when(comes_down(k) & (wrapped < chip) & (chip - wrapped <= reach))
        def _():
            for i in range(4):
                rows, share, whole = piece_of(wrapped, i, False)
                far[rows, :] = jnp.exp2(-whole) * far[rows, :] + share

        return 0

    lax.fori_loop(0, steps, visit, 0)

    for h in range(2):
        rows = pl.ds(h * both, both)
        mix[h] = (near[rows, :] + jnp.exp2(-carry[rows, :]) * far[rows, :]).astype(jnp.bfloat16)
    def mixed_at(h):
        return mixed.at[:, at(core * 256 + h * 128, 128)]

    back = [
        remote(mix.at[h, at(other * tok), :], mixed_at(h), back_send.at[h], back_recv.at[h], "sp", partner)
        for h in range(2)
    ]
    for copy in back:
        copy.start()
    pl.semaphore_wait(known.at[0], 2)
    tell(1)
    for h in range(2):
        mixed[:, at(core * 256 + h * 128, 128)] = mix[h, at(core * tok), :]
    for copy in back:
        copy.wait_recv()

    waves = chips // 4
    half_ring = chips // 2
    peers = 2 * chips
    rows, width = resid.shape
    quarter = width // 4
    half = width // 2

    def block(n, which, first=0, size=None):
        return partial.at[n, pl.ds(pl.multiple_of(which * rows, rows), rows), pl.ds(first, size or width)]

    def first_send_of(n, i):
        owner = (peer_a, peer_b, across, across)[i]
        into = (first_a, first_b)[i % 2].at[n, i // 2]
        return remote(
            block(n, owner, (i % 2) * half, half),
            into,
            first_send.at[n, i],
            first_recv.at[n, i],
            "tp",
            (peer_a, peer_b)[i % 2],
        )

    def second_send_of(n, i):
        into = (second_b, second_a)[i].at[n]
        return remote(
            summed.at[n, i], into, second_send.at[n, i], second_recv.at[n, i], "tp", (peer_b, peer_a)[i]
        )

    def sum_start(n):
        for i in (2, 3, 0, 1):
            first_send_of(n, i).start()

    def sum_middle(n):
        first_send_of(n, 2).wait_recv()
        summed[n, 0] = (
            block(n, peer_b, 0, half)[...].astype(jnp.float32) + first_a[n, 1].astype(jnp.float32)
        ).astype(jnp.bfloat16)
        second_send_of(n, 0).start()
        first_send_of(n, 3).wait_recv()
        summed[n, 1] = (
            block(n, peer_a, half, half)[...].astype(jnp.float32) + first_b[n, 1].astype(jnp.float32)
        ).astype(jnp.bfloat16)
        second_send_of(n, 1).start()

    def sum_end(n):
        first_send_of(n, 0).wait_recv()
        first_send_of(n, 1).wait_recv()
        left = block(n, tp, 0, half)[...].astype(jnp.float32) + first_a[n, 0].astype(jnp.float32)
        right = block(n, tp, half, half)[...].astype(jnp.float32) + first_b[n, 0].astype(jnp.float32)
        second_send_of(n, 0).wait_recv()
        left = left + second_b[n].astype(jnp.float32)
        second_send_of(n, 1).wait_recv()
        right = right + second_a[n].astype(jnp.float32)
        return left, right

    for copy in loads:
        copy.wait()
    for j in range(4):
        columns = pl.ds(j * quarter, quarter)
        partial[waves, :, columns] = jnp.dot(
            mixed[...], w_out[:, columns], preferred_element_type=jnp.float32
        ).astype(jnp.bfloat16)
    sum_start(waves)

    for level in range(1, levels - 1):
        pl.semaphore_wait(known.at[level], 2)
        tell(level + 1)
    sum_middle(waves)
    left, right = sum_end(waves)
    for first, part in ((0, left), (half, right)):
        columns = pl.ds(first, half)
        middle[:, columns] = (resid[:, columns].astype(jnp.float32) + part).astype(jnp.bfloat16)
    value = middle[...].astype(jnp.float32)
    value = value * lax.rsqrt(jnp.mean(value * value, axis=1, keepdims=True) + 1e-06) * gain_ref[...]
    value = value.astype(jnp.bfloat16)
    for j in range(4):
        stack[pl.ds(j * rows, rows), :] = value[:, j * quarter : (j + 1) * quarter]
    pl.semaphore_wait(known.at[levels - 1], 2)
    pl.semaphore_signal(known.at[levels], inc=1, device_id={"sp": partner}, device_id_type=MESH_ID)
    outgoing[...] = jnp.dot(spread[...], stack[...], preferred_element_type=jnp.float32).astype(jnp.bfloat16)

    def offsets(w):
        last = w == waves - 1
        far, close = half_ring - 1 - w, 1 + w
        return (far, -far, jnp.where(last, half_ring, close), jnp.where(last, 0, -close))

    def tile(x):
        return pl.ds(pl.multiple_of(x * 16, 16), 16)

    def dispatch(w, m, rel):
        target = lax.rem(chip - offsets(w)[m] + 2 * chips, chips) * 2 + lax.rem(core + rel, 2)
        return remote(
            outgoing.at[tile(target), :],
            inbox.at[w, tp, pl.ds((2 * m + rel) * 16, 16), :],
            z_send,
            z_recv.at[w, m // 2],
            "sp",
            target,
        )

    def answer(w, m, rel):
        target = lax.rem(chip + offsets(w)[m] + chips, chips) * 2 + lax.rem(core + rel, 2)
        return remote(
            reply.at[w, pl.ds((2 * m + rel) * 16, 16), :],
            returned.at[tile(me), :],
            reply_send,
            reply_recv,
            "sp",
            target,
        )

    def all_of(w, make):
        for m in range(4):
            for rel in range(2):
                if m == 3 and rel == 0:

                    @pl.when(w < waves - 1)
                    def _():
                        make(w, m, rel).start()

                else:
                    make(w, m, rel).start()

    own_in = pltpu.make_async_copy(
        outgoing.at[tile(me), :], inbox.at[waves - 1, tp, pl.ds(96, 16), :], self_sem.at[0]
    )
    own_out = pltpu.make_async_copy(
        reply.at[waves - 1, pl.ds(96, 16), :], returned.at[tile(me), :], self_sem.at[1]
    )
    pl.semaphore_wait(known.at[levels], 1)
    own_in.start()

    def send_all(w, _):
        all_of(w, dispatch)
        return 0

    lax.fori_loop(0, waves, send_all, 0)

    def part(w, owner, h):
        return inbox.at[w, owner, pl.ds(h * 64, 64), :]

    def to_a(w, h, owner):
        return remote(part(w, owner, h), part(w, owner, h), a_send.at[w, h], a_recv.at[w, h], "tp", peer_a)

    def to_b(w, h, owner):
        return remote(part(w, owner, h), part(w, owner, h), b_send.at[w, h], b_recv.at[w, h], "tp", peer_b)

    def relay_a(w, owner):
        return remote(part(w, owner, 0), part(w, owner, 0), relay_send.at[w, 0], relay_recv.at[w, 0], "tp", peer_a)

    def relay_b(w, owner):
        return remote(part(w, owner, 1), part(w, owner, 1), relay_send.at[w, 1], relay_recv.at[w, 1], "tp", peer_b)

    def landed(w, h, count):
        ref = inbox.at[w, tp, pl.ds(h * 64, count), :]
        return remote(ref, ref, z_send, z_recv.at[w, h], "sp", lax.rem(me + 1, peers))

    def forward(w):
        landed(w, 0, 64).wait_recv()
        to_a(w, 0, tp).start()
        to_b(w, 0, tp).start()

        @pl.when(w < waves - 1)
        def _():
            landed(w, 1, 64).wait_recv()

        @pl.when(w == waves - 1)
        def _():
            landed(w, 1, 48).wait_recv()
            own_in.wait()

        to_a(w, 1, tp).start()
        to_b(w, 1, tp).start()

    def pass_on(w):
        to_b(w, 0, peer_b).wait_recv()
        relay_a(w, peer_b).start()
        to_a(w, 1, peer_a).wait_recv()
        relay_b(w, peer_a).start()

    def compute(w):
        to_a(w, 0, peer_a).wait_recv()
        to_b(w, 1, peer_b).wait_recv()
        relay_a(w, across).wait_recv()
        relay_b(w, across).wait_recv()
        for j in range(4):
            turned = jnp.dot(order[0], inbox[w, j], preferred_element_type=jnp.float32).astype(jnp.bfloat16)
            for k in range(4):
                rows_in[pl.ds(j * 32, 32), pl.ds(k * quarter, quarter)] = turned[k * 32 : (k + 1) * 32]
        gate = jnp.dot(rows_in[...], w_gate[...], preferred_element_type=jnp.float32)
        lift = jnp.dot(rows_in[...], w_up[...], preferred_element_type=jnp.float32)
        hidden = (gate / (1.0 + jnp.exp(-gate)) * lift).astype(jnp.bfloat16)
        for j in range(4):
            columns = pl.ds(j * quarter, quarter)
            partial[w, :, columns] = jnp.dot(
                hidden, w_down[:, columns], preferred_element_type=jnp.float32
            ).astype(jnp.bfloat16)
        sum_start(w)

    def give_back(w):
        left, right = sum_end(w)
        left, right = left.astype(jnp.bfloat16), right.astype(jnp.bfloat16)
        whole = jnp.concatenate(
            [left[:, :quarter], left[:, quarter:], right[:, :quarter], right[:, quarter:]], axis=0
        )
        reply[w] = jnp.dot(order[1], whole, preferred_element_type=jnp.float32).astype(jnp.bfloat16)
        all_of(w, answer)

        @pl.when(w == waves - 1)
        def _():
            own_out.start()

    def drain_ring(block, _):
        for piece in range(count):

            @pl.when((block <= chip) & need_up(chip + 1, block))
            def _():
                upward(block, piece).wait_send()

            @pl.when(need_down(below, block))
            def _():
                downward(block, piece).wait_send()

        return 0

    lax.fori_loop(0, chips, drain_ring, 0)

    def turn(it, _):
        @pl.when(it < waves)
        def _():
            forward(it)

        @pl.when((it >= 2) & (it < waves + 2))
        def _():
            sum_middle(it - 2)

        @pl.when((it >= 1) & (it < waves + 1))
        def _():
            compute(it - 1)

        @pl.when(it < waves)
        def _():
            pass_on(it)

        @pl.when((it >= 2) & (it < waves + 2))
        def _():
            give_back(it - 2)

        return 0

    lax.fori_loop(0, waves + 2, turn, 0)

    rest = (peers - 1) * 16
    own_out.wait()
    everything = returned.at[pl.ds(0, rest), :]
    remote(everything, everything, reply_send, reply_recv, "sp", lax.rem(me + 1, peers)).wait_recv()
    mixed_rows = jnp.dot(weigh[0], returned[...], preferred_element_type=jnp.float32) + jnp.dot(
        weigh[1], returned[...], preferred_element_type=jnp.float32
    )
    for j in range(4):
        columns = pl.ds(j * quarter, quarter)
        out_ref[:, columns] = (
            middle[:, columns].astype(jnp.float32) + mixed_rows[j * rows : (j + 1) * rows]
        ).astype(jnp.bfloat16)

    sent = outgoing.at[pl.ds(0, rest), :]
    remote(sent, sent, z_send, z_recv.at[0, 0], "sp", lax.rem(me + 1, peers)).wait_send()
    remote(everything, everything, reply_send, reply_recv, "sp", lax.rem(me + 1, peers)).wait_send()

    def drain(w, _):
        for i in range(4):
            first_send_of(w, i).wait_send()
        for i in range(2):
            second_send_of(w, i).wait_send()

        @pl.when(w < waves)
        def _():
            for h in range(2):
                to_a(w, h, tp).wait_send()
                to_b(w, h, tp).wait_send()
            relay_a(w, peer_b).wait_send()
            relay_b(w, peer_a).wait_send()

        return 0

    lax.fori_loop(0, waves + 1, drain, 0)
    for copy in traded + back:
        copy.wait_send()


def layer(
    queries,
    keys,
    values,
    head_bias,
    documents,
    w_out,
    resid,
    norm_gain,
    expert_ids,
    expert_gates,
    w_gate,
    w_up,
    w_down,
):
    chips = lax.axis_size("sp") // 2
    tok = queries.shape[0]
    both = 2 * tok
    doc_rows = 16
    longest = chips * both * 3 // 4
    reach = (longest - 1 + both - 1) // both
    rows, width = resid.shape
    quarter, half = width // 4, width // 2
    peers = 2 * chips
    waves = chips // 4
    hidden = w_gate.shape[2]
    smem = pl.BlockSpec(memory_space=pltpu.SMEM)
    vmem = pl.BlockSpec(memory_space=pltpu.VMEM)
    hbm = pl.BlockSpec(memory_space=pl.ANY)
    dma = pltpu.SemaphoreType.DMA
    bf16, f32 = jnp.bfloat16, jnp.float32
    return pl.pallas_call(
        functools.partial(layer_kernel, chips, reach),
        out_shape=jax.ShapeDtypeStruct((rows, width), bf16),
        in_specs=[hbm] * 8 + [vmem] * 4 + [smem],
        out_specs=vmem,
        scratch_shapes=[
            pltpu.VMEM((chips, 2 * both + 2 * doc_rows, 128), bf16),
            pltpu.VMEM((2 * both, 128), bf16),
            pltpu.VMEM((doc_rows, tok), bf16),
            pltpu.VMEM((both, 128), f32),
            pltpu.VMEM((both, both), bf16),
            pltpu.VMEM((2 * both, 128), f32),
            pltpu.VMEM((2 * both, 128), f32),
            pltpu.VMEM((2 * both, 128), f32),
            pltpu.VMEM((2, both, 128), bf16),
            pltpu.VMEM((tok, 512), bf16),
            pltpu.SemaphoreType.REGULAR(((chips // 4).bit_length() + 1,)),
            dma((5,)),
            dma((5,)),
            dma((5,)),
            dma((chips, 2)),
            dma((chips, 2)),
            dma((chips, 2)),
            dma((chips, 2)),
            dma((2,)),
            dma((2,)),
            pltpu.VMEM(w_out.shape, bf16),
            pltpu.VMEM((width, hidden), bf16),
            pltpu.VMEM((width, hidden), bf16),
            pltpu.VMEM((hidden, width), bf16),
            pltpu.VMEM((rows, width), bf16),
            pltpu.VMEM((waves + 1, 4 * rows, width), bf16),
            pltpu.VMEM((waves + 1, 2, rows, half), bf16),
            pltpu.VMEM((waves + 1, 2, rows, half), bf16),
            pltpu.VMEM((waves + 1, 2, rows, half), bf16),
            pltpu.VMEM((waves + 1, rows, half), bf16),
            pltpu.VMEM((waves + 1, rows, half), bf16),
            pltpu.VMEM((rows, width), bf16),
            pltpu.VMEM((4 * rows, quarter), bf16),
            pltpu.VMEM((peers * 16, quarter), bf16),
            pltpu.VMEM((waves, 4, 128, quarter), bf16),
            pltpu.VMEM((128, width), bf16),
            pltpu.VMEM((waves, 128, quarter), bf16),
            pltpu.VMEM((peers * 16, quarter), bf16),
            pltpu.VMEM((2, 128, 128), bf16),
            pltpu.VMEM((peers * 16, 128), bf16),
            pltpu.VMEM((2, 128, peers * 16), bf16),
            pltpu.VMEM((8, 128), f32),
            dma((5,)),
            dma((2,)),
            dma,
            dma((waves, 2)),
            dma((waves, 2)),
            dma((waves, 2)),
            dma((waves, 2)),
            dma((waves, 2)),
            dma((waves, 2)),
            dma((waves, 2)),
            dma((waves + 1, 4)),
            dma((waves + 1, 4)),
            dma((waves + 1, 2)),
            dma((waves + 1, 2)),
            dma,
            dma,
        ],
        compiler_params=pltpu.CompilerParams(collective_id=0, has_side_effects=True),
        name="layer",
    )(
        queries,
        keys,
        values,
        w_out,
        resid,
        w_gate,
        w_up,
        w_down,
        documents.reshape(1, -1),
        norm_gain.reshape(1, -1),
        expert_ids.T,
        expert_gates.T,
        head_bias,
    )


def solution(mesh):
    everyone = ("grp", "sp", "tp")
    in_specs = (
        P(("grp", "sp"), "tp"),
        P(("grp", "sp"), "tp"),
        P(("grp", "sp"), "tp"),
        P("tp"),
        P(("grp", "sp")),
        P("tp", None),
        P(everyone, None),
        P(),
        P(everyone, None),
        P(everyone, None),
        P("sp", None, "tp"),
        P("sp", None, "tp"),
        P("sp", "tp", None),
    )
    return jax.shard_map(layer, mesh=mesh, in_specs=in_specs, out_specs=P(everyone, None), check_vma=False)
```
